256 devices in a mesh: sp: 64 (over z, x, core), tp: 4 (over y).
Axes of the slice: x: 4, y: 4, z: 8, core: 2. Of those that a mesh axis runs over, the one named last changes fastest.
Arguments:
- stream: bfloat16 [32768, 2048], P(('sp', 'tp')), may hold values from -6 to 6
- pool_in: bfloat16 [32768, 1024], P('sp', 'tp'), may hold values from -6 to 6
- doc_ids: int32 [32768], P('sp'), may hold values from 0 to 7, never falling along the last dimension, each value on 1 to 8192 neighbouring positions
- pool_map: bfloat16 [4, 256, 512], P('tp'), may hold values from -0.375 to 0.375
- pool_scale: float32 [2048], P('tp'), may hold values from 0.1 to 1.9
- out_weight: bfloat16 [2048, 2048], P('tp'), may hold values from -0.125 to 0.125
- norm_gain: float32 [2048], replicated, may hold values from 0.1 to 1.9
- routes: int32 [32768, 2], P('sp'), may hold values from 0 to 63, all different within a row; in each aligned block of 128 rows (0 to 127, 128 to 255, ...) at most 6 rows name the same one
- route_weight: float32 [32768, 2], P(('sp', 'tp')), may hold values from 0.2 to 1
- expert_gate: bfloat16 [64, 2048, 1024], P('sp', None, 'tp'), may hold values from -0.125 to 0.125
- expert_up: bfloat16 [64, 2048, 1024], P('sp', None, 'tp'), may hold values from -0.125 to 0.125
- expert_down: bfloat16 [64, 1024, 2048], P('sp', 'tp'), may hold values from -0.1875 to 0.1875
Outputs:
- result: bfloat16 [32768, 2048], P(('sp', 'tp'))
The draws below stay inside these ranges and needn't reach their ends.
Inputs may be any that keep to these rules, and one draw needn't show every extreme that they name: `routes`: each token names 2 different experts; in each aligned block of 128 rows no expert is named by more than 6 rows, a bound that some block reaches. `doc_ids`: never falling; each document holds at most 8192 positions.
All inputs are finite; a program needn't handle non-finite values.
Results may differ from the reference program's by a relative error of at most 0.014.
Values may be sent and summed in bfloat16 or wider, within the bound.
A program may use at most 64 MiB of HBM per device.

```python
import math
import jax
import jax.numpy as jnp
import numpy as np
from jax import lax

D = 2048
PW = 1024
GROUPS = 4
FF = 1024
TOPK = 2
DOC_COUNT = 8
GW = 256
GOUT = 512
QUART = 128
TOKENS = 32768
EXPERTS = 64
CAP = 6
FF_PART = 256
DOC_MOST = 8192
N_TP = 4


def block_levels(rng, dims, cuts, low, high):
    loudness, own = 1.0, jax.random.fold_in(rng, 6)
    for dim, blocks in cuts:
        heights = jnp.exp(jax.random.uniform(jax.random.fold_in(own, dim), (blocks,), jnp.float32, low / len(cuts), high / len(cuts)))
        loudness = loudness * jnp.repeat(heights, dims[dim] // blocks).reshape([-1 if axis == dim else 1 for axis in range(len(dims))])
    return loudness


def split_up(number_of, total, bound, lean):
    loads = [(1 << 20) // math.isqrt(rank ** lean) + 1 for rank in range(2, number_of + 1)]
    spare, holding = total - bound - (number_of - 1), [1] * (number_of - 1)
    while spare > 0:
        candidates = [i for i in range(number_of - 1) if holding[i] < bound]
        pool, budget = sum([loads[i] for i in candidates]), spare
        for i in candidates:
            addition = min(bound - holding[i], max(1, budget * loads[i] // pool), spare)
            holding[i] = holding[i] + addition
            spare = spare - addition
    return np.array([bound] + holding)


def ragged_sizes(stream_key, number_of, total, reach, lean):
    if number_of == 2:
        one = jax.random.randint(stream_key, (), max(1, total - reach), min(reach, total - 1) + 1)
        return jnp.stack([one, total - one])
    lengths = jnp.asarray(split_up(number_of, total, reach, lean), jnp.int32)
    twos = (number_of - 1) // 2
    donor, receiver = lengths[1:1 + 2 * twos:2], lengths[2:2 + 2 * twos:2]
    slack = jnp.minimum(donor - 1, reach - receiver)
    passed = jax.random.randint(jax.random.fold_in(stream_key, 1), (twos,), 0, 1 << 20) % (slack + 1)
    lengths = lengths.at[1:1 + 2 * twos:2].set(donor - passed).at[2:2 + 2 * twos:2].set(receiver + passed)
    return lengths[jax.random.permutation(jax.random.fold_in(stream_key, 2), number_of)]


def routed_block(rng, own, number, rows, number_of, top, most, skew):
    order = jax.random.permutation(rng, number_of)
    heavy_load, usual = shares(number_of, rows * top, most, skew, True), shares(number_of, rows * top, most, skew, False)
    places = jnp.arange(number_of)

    def named(tallies, rotation):
        used = int((tallies > 0).sum())
        fixed = max(1, used // 4)
        moved = fixed + (places - fixed + rotation * (used - fixed)) % max(1, number_of - fixed)
        return jnp.zeros((number_of,), jnp.int32).at[order[jnp.where(places < fixed, places, moved)]].set(jnp.asarray(tallies, jnp.int32))

    tallies = jnp.where(number % 4 == 0, named(heavy_load, number // 4), named(usual, number - number // 4 - 1))
    mixed = jax.random.permutation(jax.random.fold_in(own, 3), number_of)
    giver, sink = mixed[0:number_of // 2 * 2:2], mixed[1:number_of // 2 * 2:2]
    margin = jnp.minimum(tallies[giver] - 1, most - tallies[sink]) // 2
    margin = jnp.where((giver == order[0]) | (sink == order[0]) | (tallies[sink] == 0), 0, jnp.maximum(margin, 0))
    moved = jax.random.randint(jax.random.fold_in(own, 4), (number_of // 2,), 0, 1 << 20) % (margin + 1)
    tallies = tallies.at[giver].add(-moved).at[sink].add(moved)
    items = jnp.searchsorted(jnp.cumsum(tallies), jnp.arange(rows * top), side="right").astype(jnp.int32)
    grid = items.reshape(top, rows).T
    grid = grid[jax.random.permutation(jax.random.fold_in(own, 1), rows)]
    rotation = jax.random.randint(jax.random.fold_in(own, 2), (rows, 1), 0, top)
    return jnp.take_along_axis(grid, (jnp.arange(top)[None, :] + rotation) % top, axis=1)


def shares(number_of, total, bound, skew, full):
    portions = [(1 << 20) // math.isqrt(grade ** skew) + 1 for grade in range(1, number_of + 1)]
    largest = bound if full else min(bound, max(-(-total // number_of), total * portions[0] // sum(portions)))
    least = 1 if total - largest >= number_of - 1 else 0
    given, rest = [largest] + [least] * (number_of - 1), total - largest - least * (number_of - 1)
    while rest > 0:
        movable = [i for i in range(1, number_of) if given[i] < largest] or [i for i in range(1, number_of) if given[i] < bound]
        whole, left = sum([portions[i] for i in movable]), rest
        for i in movable:
            more = min(bound - given[i], max(1, left * portions[i] // whole), rest)
            given[i] = given[i] + more
            rest = rest - more
    return np.array(given)


def normal_values(stream_key, shape, width, limit, pieces=(), kind=jnp.bfloat16):
    drawn = width * jax.random.normal(stream_key, shape, jnp.float32)
    if pieces:
        drawn = drawn * block_levels(stream_key, shape, pieces, -0.22, 0.18)
    return jnp.clip(drawn, -limit, limit).astype(kind)


def setup_inputs(seed: int = 0) -> dict:
    streams_of = jax.random.split(jax.random.key(seed), 13)
    stream = normal_values(streams_of[0], (TOKENS, D), 1.0, 6.0, ((0, 256),))
    pool_in = normal_values(streams_of[1], (TOKENS, PW), 1.0, 6.0, ((0, 64), (1, 4)))
    doc_ids = jnp.searchsorted(jnp.cumsum(ragged_sizes(streams_of[2], DOC_COUNT, TOKENS, DOC_MOST, 1)), jnp.arange(TOKENS), side="right").astype(jnp.int32)
    pool_map = normal_values(streams_of[3], (GROUPS, GW, GOUT), GW ** -0.5, 0.375, ((0, 4),))
    pool_scale = jnp.clip(1.0 + 0.18 * jax.random.normal(streams_of[4], (D,), jnp.float32), 0.1, 1.9)
    out_weight = normal_values(streams_of[5], (D, D), D ** -0.5, 0.125, ((0, 4),))
    norm_gain = jnp.clip(1.0 + 0.18 * jax.random.normal(streams_of[6], (D,), jnp.float32), 0.1, 1.9)
    routes_keys = jax.random.split(jax.random.fold_in(streams_of[7], 1), TOKENS // QUART)
    routes_turns = jax.random.permutation(jax.random.fold_in(streams_of[7], 3), TOKENS // QUART)
    routes = jax.vmap(lambda own, number: routed_block(jax.random.fold_in(streams_of[7], 2), own, number, QUART, EXPERTS, TOPK, CAP, 1))(routes_keys, routes_turns).reshape((TOKENS, TOPK))
    route_weight = jnp.clip(0.2 + 0.8 * jax.random.uniform(streams_of[8], (TOKENS, TOPK), jnp.float32) ** block_levels(streams_of[8], (TOKENS, TOPK), ((0, 256),), -0.2, 0.2), 0.2, 1.0)
    expert_gate = normal_values(streams_of[9], (EXPERTS, D, FF), D ** -0.5, 0.125, ((0, 64), (2, 4)))
    expert_up = normal_values(streams_of[10], (EXPERTS, D, FF), D ** -0.5, 0.125, ((0, 64), (2, 4)))
    expert_down = normal_values(streams_of[11], (EXPERTS, FF, D), FF ** -0.5, 0.1875, ((0, 64), (1, 4)))
    return dict(stream=stream, pool_in=pool_in, doc_ids=doc_ids, pool_map=pool_map, pool_scale=pool_scale, out_weight=out_weight, norm_gain=norm_gain, routes=routes, route_weight=route_weight, expert_gate=expert_gate, expert_up=expert_up, expert_down=expert_down)


EPS = 1e-06

def reference(stream, pool_in, doc_ids, pool_map, pool_scale, out_weight, norm_gain, routes, route_weight, expert_gate, expert_up, expert_down):
    total_rows = pool_in.shape[0]
    positions = jnp.arange(total_rows, dtype=jnp.int32)
    starts_here = jnp.concatenate([jnp.ones((1,), jnp.bool_), doc_ids[1:] != doc_ids[:-1]])
    doc_start = lax.cummax(jnp.where(starts_here, positions, 0).astype(jnp.int32), axis=0)
    source_rows = pool_in.astype(jnp.float32)
    branch_parts = []
    for group_index in range(GROUPS):
        window = 2 << group_index
        group_cols = source_rows[:, group_index * GW:(group_index + 1) * GW]
        running = jnp.zeros_like(group_cols)
        counts = jnp.zeros((total_rows,), jnp.float32)
        for offset in range(window):
            shifted = jnp.concatenate([jnp.zeros((offset, GW), jnp.float32), group_cols[:total_rows - offset]], axis=0)
            in_window = positions - offset >= doc_start
            running = running + jnp.where(in_window[:, None], shifted, 0.0)
            counts = counts + in_window.astype(jnp.float32)
        pooled = (running / counts[:, None] - group_cols).astype(jnp.bfloat16)
        mapped = jnp.dot(pooled, pool_map[group_index], preferred_element_type=jnp.float32)
        branch_parts.append((mapped * pool_scale[group_index * GOUT:(group_index + 1) * GOUT]).astype(jnp.bfloat16))
    branch = jnp.concatenate(branch_parts, axis=1)
    mixed_rows = (stream.astype(jnp.float32) + jnp.dot(branch, out_weight, preferred_element_type=jnp.float32)).astype(jnp.bfloat16)
    mixed_up = mixed_rows.astype(jnp.float32)
    normed = (mixed_up * lax.rsqrt(lax.optimization_barrier(jnp.mean(mixed_up * mixed_up, axis=1, keepdims=True)) + EPS) * norm_gain).astype(jnp.bfloat16)
    block_count = total_rows // QUART
    flattened = routes.reshape(-1).astype(jnp.int32)
    one_hot = (flattened[:, None] == jnp.arange(EXPERTS, dtype=jnp.int32)[None, :]).astype(jnp.int32)
    blocked = one_hot.reshape(block_count, QUART * TOPK, EXPERTS)
    ranking = lax.optimization_barrier(jnp.sum((jnp.cumsum(blocked, axis=1) - blocked) * blocked, axis=2)).reshape(-1).astype(jnp.int32)
    assign_ids = jnp.arange(total_rows * TOPK, dtype=jnp.int32)
    block_ids = (assign_ids // (QUART * TOPK)).astype(jnp.int32)
    target_slot = ((flattened * block_count + block_ids) * CAP + ranking).astype(jnp.int32)
    per_expert = block_count * CAP
    slot_token = jnp.zeros((EXPERTS * per_expert,), jnp.int32).at[target_slot].set((assign_ids // TOPK).astype(jnp.int32))
    slot_weight = jnp.zeros((EXPERTS * per_expert,), jnp.float32).at[target_slot].set(route_weight.reshape(-1))

    def one_expert(accumulated, expert_index):
        begin_slot = (expert_index * per_expert).astype(jnp.int32)
        tokens_here = lax.dynamic_slice_in_dim(slot_token, begin_slot, per_expert)
        weights_here = lax.dynamic_slice_in_dim(slot_weight, begin_slot, per_expert)
        inputs = normed[tokens_here]
        gate_pre = jnp.dot(inputs, expert_gate[expert_index], preferred_element_type=jnp.float32)
        up_pre = jnp.dot(inputs, expert_up[expert_index], preferred_element_type=jnp.float32)
        hidden = (jax.nn.silu(gate_pre) * up_pre).astype(jnp.bfloat16)
        down_rows = expert_down[expert_index]
        summed = jnp.zeros((per_expert, D), jnp.float32)
        for part_index in range(N_TP):
            part_begin = part_index * FF_PART
            part_out = jnp.dot(hidden[:, part_begin:part_begin + FF_PART], down_rows[part_begin:part_begin + FF_PART], preferred_element_type=jnp.float32).astype(jnp.bfloat16)
            summed = summed + lax.optimization_barrier(part_out).astype(jnp.float32)
        expert_out = lax.optimization_barrier(summed.astype(jnp.bfloat16)).astype(jnp.float32)
        return (accumulated.at[tokens_here].add(weights_here[:, None] * expert_out), None)
    accumulated, unused_out = lax.scan(one_expert, jnp.zeros((total_rows, D), jnp.float32), jnp.arange(EXPERTS, dtype=jnp.int32))
    return (mixed_up + accumulated).astype(jnp.bfloat16)
```

```python
import jax
import jax.numpy as jnp
from jax import lax
from jax.sharding import PartitionSpec as P

SPAN = 16


EPS = 1e-06


def passed_along(value, axis, by):
    length = lax.axis_size(axis)
    pairs = [(i, i + by) for i in range(length) if 0 <= i + by < length]
    return lax.ppermute(value, axis, pairs)


def cut_along(value, dim, length):
    before, after = (value.shape[:dim], value.shape[dim + 1 :])
    return jnp.moveaxis(value.reshape(*before, length, -1, *after), dim, 0)


def sum_at_owner(value, axis, dim):
    length = lax.axis_size(axis)
    tiles = lax.all_to_all(cut_along(value, dim, length), axis, 0, 0, tiled=True)
    return jnp.sum(tiles.astype(jnp.float32), axis=0)


def slot_table(route_block, expert_count, capacity, top_count):
    flattened = route_block.reshape(-1)
    one_hot = (flattened[:, None] == jnp.arange(expert_count, dtype=jnp.int32)[None, :]).astype(
        jnp.int32
    )
    ranking = jnp.sum((jnp.cumsum(one_hot, axis=0) - one_hot) * one_hot, axis=1)
    target_slot = flattened * capacity + ranking
    matches = target_slot[None, :] == jnp.arange(expert_count * capacity, dtype=jnp.int32)[:, None]
    sources = jnp.sum(
        jnp.where(matches, jnp.arange(flattened.shape[0], dtype=jnp.int32)[None, :], 0), axis=1
    )
    filled = jnp.any(matches, axis=1)
    return (target_slot, sources // top_count, filled)


def per_device(
    stream,
    pool_in,
    doc_ids,
    pool_map,
    pool_scale,
    out_weight,
    norm_gain,
    routes,
    route_weight,
    expert_gate,
    expert_up,
    expert_down,
):
    row_count = pool_in.shape[0]
    model_width = stream.shape[1]
    top_count = routes.shape[1]
    tp_count = lax.axis_size("tp")
    expert_count = lax.axis_size("sp")
    quarter = row_count // tp_count
    capacity = max(2, 3 * top_count * quarter // (2 * expert_count))
    all_gate = lax.all_gather(expert_gate, "tp", axis=0, tiled=True)
    all_up = lax.all_gather(expert_up, "tp", axis=0, tiled=True)
    all_down = lax.all_gather(expert_down, "tp", axis=0, tiled=True)
    reach_rows = SPAN - 1
    tail_rows = (
        pool_in[row_count - reach_rows :],
        doc_ids[row_count - reach_rows :].astype(jnp.bfloat16),
    )
    prior_rows, prior_docs = passed_along((tail_rows[0], tail_rows[1]), "sp", 1)
    extended = jnp.concatenate([prior_rows, pool_in], axis=0).astype(jnp.float32)
    extended_docs = jnp.concatenate([prior_docs.astype(jnp.float32), doc_ids.astype(jnp.float32)])
    own_docs = doc_ids.astype(jnp.float32)
    window = jnp.left_shift(jnp.int32(2), lax.axis_index("tp"))
    positions = lax.axis_index("sp") * row_count + jnp.arange(row_count, dtype=jnp.int32)
    running = jnp.zeros(pool_in.shape, jnp.float32)
    counts = jnp.zeros((row_count,), jnp.float32)
    for offset in range(reach_rows + 1):
        begin_row = reach_rows - offset
        piece_rows = extended[begin_row : begin_row + row_count]
        piece_docs = extended_docs[begin_row : begin_row + row_count]
        in_window = (offset < window) & (positions - offset >= 0) & (piece_docs == own_docs)
        running = running + jnp.where(in_window[:, None], piece_rows, 0.0)
        counts = counts + in_window.astype(jnp.float32)
    pooled = (running / counts[:, None] - pool_in.astype(jnp.float32)).astype(jnp.bfloat16)
    branch = (jnp.dot(pooled, pool_map[0], preferred_element_type=jnp.float32) * pool_scale).astype(
        jnp.bfloat16
    )
    projected = sum_at_owner(
        jnp.dot(branch, out_weight, preferred_element_type=jnp.float32).astype(jnp.bfloat16),
        "tp",
        0,
    )
    mixed_rows = (stream.astype(jnp.float32) + projected).astype(jnp.bfloat16)
    mixed_up = mixed_rows.astype(jnp.float32)
    normed = (
        mixed_up * lax.rsqrt(jnp.mean(mixed_up * mixed_up, axis=1, keepdims=True) + EPS) * norm_gain
    ).astype(jnp.bfloat16)
    own_routes = lax.dynamic_slice_in_dim(routes, lax.axis_index("tp") * quarter, quarter, 0)
    own_slots, own_sources, own_filled = slot_table(own_routes, expert_count, capacity, top_count)
    token_index = own_sources.reshape(expert_count, 1, capacity)
    filled_slots = own_filled.reshape(expert_count, 1, capacity)
    dispatch = jnp.where(filled_slots[..., None], normed[token_index], jnp.zeros((), jnp.bfloat16))
    arrived = lax.all_to_all(dispatch, "sp", split_axis=0, concat_axis=0, tiled=True)
    stacked = arrived.reshape(-1, model_width)
    expert_sum = jnp.zeros(stacked.shape, jnp.float32)
    for part in range(tp_count):
        gate_pre = jnp.dot(stacked, all_gate[part], preferred_element_type=jnp.float32)
        up_pre = jnp.dot(stacked, all_up[part], preferred_element_type=jnp.float32)
        hidden = (jax.nn.silu(gate_pre) * up_pre).astype(jnp.bfloat16)
        part_out = jnp.dot(hidden, all_down[part], preferred_element_type=jnp.float32)
        expert_sum = expert_sum + part_out.astype(jnp.bfloat16).astype(jnp.float32)
    summed = expert_sum.astype(jnp.bfloat16).reshape(arrived.shape)
    returned = lax.all_to_all(summed, "sp", split_axis=0, concat_axis=0, tiled=True)
    outputs = returned.reshape(expert_count * capacity, model_width)
    picked = outputs[own_slots].astype(jnp.float32).reshape(quarter, top_count, model_width)
    combined = jnp.sum(route_weight[:, :, None] * picked, axis=1)
    return (mixed_up + combined).astype(jnp.bfloat16)


def solution(mesh):
    in_specs = (
        P(("sp", "tp"), None),
        P("sp", "tp"),
        P("sp"),
        P("tp", None, None),
        P("tp"),
        P("tp", None),
        P(),
        P("sp", None),
        P(("sp", "tp"), None),
        P("sp", None, "tp"),
        P("sp", None, "tp"),
        P("sp", "tp", None),
    )
    out_specs = P(("sp", "tp"), None)
    return jax.shard_map(
        per_device, mesh=mesh, in_specs=in_specs, out_specs=out_specs, check_vma=False
    )
```

```python
import functools

import jax
import jax.numpy as jnp
from jax import lax
from jax.experimental import pallas as pl
from jax.experimental.pallas import tpu as pltpu
from jax.sharding import PartitionSpec as P

MESH = pl.DeviceIdType.MESH
SPAN = 16
EPS = 1e-06
LANES = 128
HALVES = 2


def passed_along(value, axis, by):
    length = lax.axis_size(axis)
    pairs = [(i, i + by) for i in range(length) if 0 <= i + by < length]
    return lax.ppermute(value, axis, pairs)


def slot_table(route_block, expert_count, capacity, top_count):
    flattened = route_block.reshape(-1)
    one_hot = (flattened[:, None] == jnp.arange(expert_count, dtype=jnp.int32)[None, :]).astype(
        jnp.int32
    )
    ranking = jnp.sum((jnp.cumsum(one_hot, axis=0) - one_hot) * one_hot, axis=1)
    target_slot = flattened * capacity + ranking
    matches = target_slot[None, :] == jnp.arange(expert_count * capacity, dtype=jnp.int32)[:, None]
    sources = jnp.sum(
        jnp.where(matches, jnp.arange(flattened.shape[0], dtype=jnp.int32)[None, :], 0), axis=1
    )
    return (target_slot, sources // top_count)


def layer_kernel(
    experts,
    capacity,
    tp_count,
    source_ref,
    slot_ref,
    weight_ref,
    part_hbm,
    stream_hbm,
    gain_ref,
    gate_hbm,
    up_hbm,
    down_hbm,
    out_ref,
    tiles,
    stream_v,
    mixed,
    tokens,
    rounded,
    packed,
    arrived,
    wide,
    inputs,
    all_gate,
    all_up,
    all_down,
    hidden,
    shaped,
    sending,
    returned,
    picked_from,
    combined,
    local_sem,
    tile_send,
    tile_recv,
    row_send,
    row_recv,
    out_send,
    out_recv,
    own_send,
    own_recv,
    fwd_send,
    fwd_recv,
):
    sp, tp = lax.axis_index("sp"), lax.axis_index("tp")
    above, below, across = (tp + 1) % tp_count, (tp + tp_count - 1) % tp_count, (tp + 2) % tp_count
    rows, width = stream_v.shape
    blocks = width // LANES
    slots = experts * capacity
    depth = width // HALVES
    ff_part = hidden.shape[2]
    ff_half = ff_part // HALVES
    columns = width // HALVES
    col_blocks = columns // LANES

    def remote(src, dst, send, recv, target):
        return pltpu.make_async_remote_copy(
            src_ref=src,
            dst_ref=dst,
            send_sem=send,
            recv_sem=recv,
            device_id=target,
            device_id_type=MESH,
        )

    barrier = pltpu.get_barrier_semaphore()
    for step in range(1, tp_count):
        pl.semaphore_signal(
            barrier, inc=1, device_id=(sp, (tp + step) % tp_count), device_id_type=MESH
        )

    @pl.loop(1, experts)
    def _(step):
        pl.semaphore_signal(
            barrier, inc=1, device_id=((sp + step) % experts, tp), device_id_type=MESH
        )

    loads = [
        pltpu.make_async_copy(part_hbm.at[tp], tiles.at[tp], local_sem.at[0]),
        pltpu.make_async_copy(stream_hbm, stream_v, local_sem.at[1]),
        pltpu.make_async_copy(gate_hbm, all_gate.at[tp], local_sem.at[2]),
        pltpu.make_async_copy(up_hbm, all_up.at[tp], local_sem.at[3]),
        pltpu.make_async_copy(down_hbm, all_down.at[tp], local_sem.at[4]),
    ]
    for load in loads:
        load.start()
    pl.semaphore_wait(barrier, experts - 1 + tp_count - 1)

    for step in (1, 3, 2):
        owner = (tp + step) % tp_count
        remote(part_hbm.at[owner], tiles.at[tp], tile_send, tile_recv, (sp, owner)).start()

    def region(which, block, half):
        if which == 0:
            return all_gate.at[block, pl.ds(half * depth, depth)]
        if which == 1:
            return all_up.at[block, pl.ds(half * depth, depth)]
        return all_down.at[block, :, pl.ds(half * columns, columns)]

    def own_source(which, half):
        if which == 0:
            return gate_hbm.at[pl.ds(half * depth, depth)]
        if which == 1:
            return up_hbm.at[pl.ds(half * depth, depth)]
        return down_hbm.at[:, pl.ds(half * columns, columns)]

    def own_copy(which, half, way):
        target = above if way == 0 else below
        return remote(
            own_source(which, half),
            region(which, tp, half),
            own_send.at[way, which, half],
            own_recv.at[way, which, half],
            (sp, target),
        )

    def send_own(which, half):
        for way in range(2):
            own_copy(which, half, way).start()

    def wait_own(which, half, way):
        own_copy(which, half, way).wait_recv()

    def fwd_copy(which, part, way):
        block = below if way == 0 else above
        half = 1 - way
        if which == 2:
            ref = all_down.at[block, pl.ds(half * ff_half, ff_half), pl.ds(part * columns, columns)]
        else:
            ref = region(which, block, half)
        target = above if way == 0 else below
        return remote(
            ref, ref, fwd_send.at[way, which, part], fwd_recv.at[way, which, part], (sp, target)
        )

    for which in range(2):
        for half in range(HALVES):
            send_own(which, half)

    loads[0].wait()
    loads[1].wait()
    summed_tiles = remote(
        tiles.at[pl.ds(0, tp_count - 1)],
        tiles.at[pl.ds(0, tp_count - 1)],
        tile_send,
        tile_recv,
        (sp, above),
    )
    summed_tiles.wait_recv()

    step_rows = 16

    @pl.loop(0, rows // step_rows)
    def _(i):
        at = pl.ds(pl.multiple_of(i * step_rows, step_rows), step_rows)
        total = tiles[0, at, :].astype(jnp.float32)
        for k in range(1, tp_count):
            total = total + tiles[k, at, :].astype(jnp.float32)
        here = (stream_v[at, :].astype(jnp.float32) + total).astype(jnp.bfloat16)
        here = here.astype(jnp.float32)
        mixed[at, :] = here
        scale = lax.rsqrt(jnp.mean(here * here, axis=1, keepdims=True) + EPS)
        normed = here * scale * gain_ref[...]
        for c in range(blocks):
            tokens[pl.ds(i * (step_rows * blocks) + c, step_rows, stride=blocks), :] = normed[
                :, c * LANES : (c + 1) * LANES
            ]

    @pl.loop(0, rows, unroll=4)
    def _(t):
        rounded[t] = tokens[pl.ds(pl.multiple_of(t * blocks, blocks), blocks), :].astype(
            jnp.bfloat16
        )

    @pl.loop(0, slots, unroll=4)
    def _(s):
        packed[s] = rounded[source_ref[s]]

    @pl.loop(1, experts)
    def _(step):
        peer = (sp + step) % experts
        remote(
            packed.at[pl.ds(peer * capacity, capacity)],
            arrived.at[pl.ds(sp * capacity, capacity)],
            row_send,
            row_recv,
            (peer, tp),
        ).start()

    @pl.loop(0, capacity)
    def _(r):
        arrived[sp * capacity + r] = packed[sp * capacity + r]

    for which in range(2):
        wait_own(which, 1, 0)
        fwd_copy(which, 0, 0).start()
        wait_own(which, 0, 1)
        fwd_copy(which, 0, 1).start()
        wait_own(which, 0, 0)
        wait_own(which, 1, 1)
    for half in range(HALVES):
        send_own(2, half)

    all_rows = remote(
        packed.at[pl.ds(0, (experts - 1) * capacity)],
        arrived.at[pl.ds(0, (experts - 1) * capacity)],
        row_send,
        row_recv,
        (sp, above),
    )
    all_rows.wait_recv()

    @pl.loop(0, slots, unroll=4)
    def _(s):
        wide[pl.ds(pl.multiple_of(s * blocks, blocks), blocks), :] = arrived[s].astype(jnp.float32)

    for c in range(blocks):
        inputs[:, c * LANES : (c + 1) * LANES] = wide[pl.ds(c, slots, stride=blocks), :].astype(
            jnp.bfloat16
        )

    loads[2].wait()
    loads[3].wait()
    loads[4].wait()

    def run_hidden(block):
        gate_pre = jnp.dot(inputs[...], all_gate[block], preferred_element_type=jnp.float32)
        up_pre = jnp.dot(inputs[...], all_up[block], preferred_element_type=jnp.float32)
        hidden[block] = (jax.nn.silu(gate_pre) * up_pre).astype(jnp.bfloat16)

    run_hidden(tp)
    run_hidden(below)
    run_hidden(above)
    for which in range(2):
        for way in range(2):
            fwd_copy(which, 0, way).wait_recv()
    run_hidden(across)

    row_step = 128
    for half in range(HALVES):
        for way in range(2):
            wait_own(2, half, way)
            fwd_copy(2, half, way).start()
        for way in range(2):
            fwd_copy(2, half, way).wait_recv()

        @pl.loop(0, slots // row_step)
        def _(i):
            at = pl.ds(pl.multiple_of(i * row_step, row_step), row_step)
            total = jnp.zeros((row_step, columns), jnp.float32)
            for block in range(tp_count):
                piece = jnp.dot(
                    hidden[block, at, :],
                    all_down[block, :, half * columns : (half + 1) * columns],
                    preferred_element_type=jnp.float32,
                )
                total = total + piece.astype(jnp.bfloat16).astype(jnp.float32)
            for c in range(col_blocks):
                shaped[pl.ds(i * (row_step * col_blocks) + c, row_step, stride=col_blocks), :] = (
                    total[:, c * LANES : (c + 1) * LANES]
                )

        lines = capacity * col_blocks

        @pl.loop(0, experts)
        def _(j):
            sending[half, j] = shaped[pl.ds(pl.multiple_of(j * lines, lines), lines), :].astype(
                jnp.bfloat16
            )

        @pl.loop(1, experts)
        def _(step):
            peer = (sp + step) % experts
            remote(
                sending.at[half, peer],
                returned.at[half, sp],
                out_send.at[half],
                out_recv.at[half],
                (peer, tp),
            ).start()

        returned[half, sp] = sending[half, sp]

    def all_out(half):
        return remote(
            sending.at[half, pl.ds(0, experts - 1)],
            returned.at[half, pl.ds(0, experts - 1)],
            out_send.at[half],
            out_recv.at[half],
            (sp, above),
        )

    for half in range(HALVES):
        all_out(half).wait_recv()

        @pl.loop(0, experts)
        def _(j):
            picked_from[pl.ds(j * capacity, capacity)] = (
                returned[half, j].astype(jnp.float32).reshape(capacity, col_blocks, LANES)
            )

        @pl.loop(0, rows, unroll=4)
        def _(t):
            combined[pl.ds(pl.multiple_of(t * col_blocks, col_blocks), col_blocks), :] = (
                weight_ref[2 * t] * picked_from[slot_ref[2 * t]]
                + weight_ref[2 * t + 1] * picked_from[slot_ref[2 * t + 1]]
            )

        for c in range(col_blocks):
            at = slice(half * columns + c * LANES, half * columns + (c + 1) * LANES)
            out_ref[:, at] = (
                mixed[:, at] + combined[pl.ds(c, rows, stride=col_blocks), :]
            ).astype(jnp.bfloat16)

    summed_tiles.wait_send()
    all_rows.wait_send()
    for half in range(HALVES):
        all_out(half).wait_send()
        for way in range(2):
            for which in range(3):
                own_copy(which, half, way).wait_send()
    for way in range(2):
        for half in range(HALVES):
            fwd_copy(2, half, way).wait_send()
        fwd_copy(0, 0, way).wait_send()
        fwd_copy(1, 0, way).wait_send()


def per_device(
    stream,
    pool_in,
    doc_ids,
    pool_map,
    pool_scale,
    out_weight,
    norm_gain,
    routes,
    route_weight,
    expert_gate,
    expert_up,
    expert_down,
):
    row_count = pool_in.shape[0]
    model_width = stream.shape[1]
    top_count = routes.shape[1]
    tp_count = lax.axis_size("tp")
    expert_count = lax.axis_size("sp")
    quarter = row_count // tp_count
    capacity = max(2, 3 * top_count * quarter // (2 * expert_count))
    ff_part = expert_gate.shape[2]
    reach_rows = SPAN - 1
    tail_rows = (
        pool_in[row_count - reach_rows :],
        doc_ids[row_count - reach_rows :].astype(jnp.bfloat16),
    )
    prior_rows, prior_docs = passed_along((tail_rows[0], tail_rows[1]), "sp", 1)
    extended = jnp.concatenate([prior_rows, pool_in], axis=0).astype(jnp.float32)
    extended_docs = jnp.concatenate([prior_docs.astype(jnp.float32), doc_ids.astype(jnp.float32)])
    own_docs = doc_ids.astype(jnp.float32)
    window = jnp.left_shift(jnp.int32(2), lax.axis_index("tp"))
    positions = lax.axis_index("sp") * row_count + jnp.arange(row_count, dtype=jnp.int32)
    running = jnp.zeros(pool_in.shape, jnp.float32)
    counts = jnp.zeros((row_count,), jnp.float32)
    for offset in range(reach_rows + 1):
        begin_row = reach_rows - offset
        piece_rows = extended[begin_row : begin_row + row_count]
        piece_docs = extended_docs[begin_row : begin_row + row_count]
        in_window = (offset < window) & (positions - offset >= 0) & (piece_docs == own_docs)
        running = running + jnp.where(in_window[:, None], piece_rows, 0.0)
        counts = counts + in_window.astype(jnp.float32)
    pooled = (running / counts[:, None] - pool_in.astype(jnp.float32)).astype(jnp.bfloat16)
    branch = (jnp.dot(pooled, pool_map[0], preferred_element_type=jnp.float32) * pool_scale).astype(
        jnp.bfloat16
    )
    partial = jnp.dot(branch, out_weight, preferred_element_type=jnp.float32).astype(jnp.bfloat16)
    partial = partial.reshape(tp_count, quarter, model_width)

    own_routes = lax.dynamic_slice_in_dim(routes, lax.axis_index("tp") * quarter, quarter, 0)
    own_slots, own_sources = slot_table(own_routes, expert_count, capacity, top_count)

    slots = expert_count * capacity
    blocks = model_width // LANES
    half_blocks = blocks // HALVES
    bf16, f32 = jnp.bfloat16, jnp.float32
    vmem, dma = pltpu.VMEM, pltpu.SemaphoreType.DMA
    smem_spec = pl.BlockSpec(memory_space=pltpu.SMEM)
    any_spec = pl.BlockSpec(memory_space=pl.ANY)
    vmem_spec = pl.BlockSpec(memory_space=pltpu.VMEM)
    return pl.pallas_call(
        functools.partial(layer_kernel, expert_count, capacity, tp_count),
        out_shape=jax.ShapeDtypeStruct((quarter, model_width), bf16),
        in_specs=[smem_spec] * 3 + [any_spec] * 2 + [vmem_spec] + [any_spec] * 3,
        out_specs=vmem_spec,
        scratch_shapes=[
            vmem((tp_count, quarter, model_width), bf16),
            vmem((quarter, model_width), bf16),
            vmem((quarter, model_width), f32),
            vmem((quarter * blocks, LANES), f32),
            vmem((quarter, blocks, LANES), bf16),
            vmem((slots, blocks, LANES), bf16),
            vmem((slots, blocks, LANES), bf16),
            vmem((slots * blocks, LANES), f32),
            vmem((slots, model_width), bf16),
            vmem((tp_count, model_width, ff_part), bf16),
            vmem((tp_count, model_width, ff_part), bf16),
            vmem((tp_count, ff_part, model_width), bf16),
            vmem((tp_count, slots, ff_part), bf16),
            vmem((slots * half_blocks, LANES), f32),
            vmem((HALVES, expert_count, capacity * half_blocks, LANES), bf16),
            vmem((HALVES, expert_count, capacity * half_blocks, LANES), bf16),
            vmem((slots, half_blocks, LANES), f32),
            vmem((quarter * half_blocks, LANES), f32),
            dma((5,)),
            dma,
            dma,
            dma,
            dma,
            dma((HALVES,)),
            dma((HALVES,)),
            dma((2, 3, HALVES)),
            dma((2, 3, HALVES)),
            dma((2, 3, HALVES)),
            dma((2, 3, HALVES)),
        ],
        compiler_params=pltpu.CompilerParams(
            collective_id=0, has_side_effects=True, vmem_limit_bytes=56 * 1024 * 1024
        ),
    )(
        own_sources,
        own_slots,
        route_weight.reshape(-1),
        partial,
        stream,
        norm_gain.reshape(1, -1),
        expert_gate[0],
        expert_up[0],
        expert_down[0],
    )


def solution(mesh):
    in_specs = (
        P(("sp", "tp"), None),
        P("sp", "tp"),
        P("sp"),
        P("tp", None, None),
        P("tp"),
        P("tp", None),
        P(),
        P("sp", None),
        P(("sp", "tp"), None),
        P("sp", None, "tp"),
        P("sp", None, "tp"),
        P("sp", "tp", None),
    )
    out_specs = P(("sp", "tp"), None)
    return jax.shard_map(
        per_device, mesh=mesh, in_specs=in_specs, out_specs=out_specs, check_vma=False
    )
```

```python
import functools

import jax
import jax.numpy as jnp
from jax import lax
from jax.experimental import pallas as pl
from jax.experimental.pallas import tpu as pltpu
from jax.sharding import PartitionSpec as P

MESH = pl.DeviceIdType.MESH
EPS = 1e-06
LANES = 128
HALVES = 2
CHUNKS = 4
LINES = 8


def slot_table(route_block, expert_count, capacity, top_count):
    flattened = route_block.reshape(-1)
    one_hot = (flattened[:, None] == jnp.arange(expert_count, dtype=jnp.int32)[None, :]).astype(
        jnp.int32
    )
    ranking = jnp.sum((jnp.cumsum(one_hot, axis=0) - one_hot) * one_hot, axis=1)
    target_slot = flattened * capacity + ranking
    matches = target_slot[None, :] == jnp.arange(expert_count * capacity, dtype=jnp.int32)[:, None]
    sources = jnp.sum(
        jnp.where(matches, jnp.arange(flattened.shape[0], dtype=jnp.int32)[None, :], 0), axis=1
    )
    return (target_slot, sources // top_count)


def layer_kernel(
    experts,
    capacity,
    tp_count,
    source_ref,
    slot_ref,
    weight_ref,
    docs_ref,
    pool_hbm,
    map_hbm,
    scale_ref,
    project_hbm,
    stream_hbm,
    gain_ref,
    gate_hbm,
    up_hbm,
    down_hbm,
    out_ref,
    pool_rows,
    docs,
    pool_map,
    project,
    partial,
    tiles,
    stream_v,
    mixed,
    tokens,
    rounded,
    packed,
    arrived,
    wide,
    inputs,
    all_gate,
    all_up,
    all_down,
    hidden,
    shaped,
    sending,
    returned,
    picked_from,
    combined,
    local_sem,
    prior_send,
    prior_recv,
    tile_send,
    tile_recv,
    row_send,
    row_recv,
    out_send,
    out_recv,
    own_send,
    own_recv,
    fwd_send,
    fwd_recv,
):
    sp, tp = lax.axis_index("sp"), lax.axis_index("tp")
    above, below, across = (tp + 1) % tp_count, (tp + tp_count - 1) % tp_count, (tp + 2) % tp_count
    rows, width = stream_v.shape
    blocks = width // LANES
    slots = experts * capacity
    depth = width // HALVES
    ff_part = hidden.shape[2]
    ff_half = ff_part // HALVES
    columns = width // CHUNKS
    col_blocks = columns // LANES

    def remote(src, dst, send, recv, target):
        return pltpu.make_async_remote_copy(
            src_ref=src,
            dst_ref=dst,
            send_sem=send,
            recv_sem=recv,
            device_id=target,
            device_id_type=MESH,
        )

    barrier = pltpu.get_barrier_semaphore()
    for step in range(1, tp_count):
        pl.semaphore_signal(
            barrier, inc=1, device_id=(sp, (tp + step) % tp_count), device_id_type=MESH
        )

    @pl.loop(1, experts)
    def _(step):
        pl.semaphore_signal(
            barrier, inc=1, device_id=((sp + step) % experts, tp), device_id_type=MESH
        )

    loads = [
        pltpu.make_async_copy(pool_hbm, pool_rows.at[pl.ds(1, tp_count)], local_sem.at[0]),
        pltpu.make_async_copy(stream_hbm, stream_v, local_sem.at[1]),
        pltpu.make_async_copy(gate_hbm, all_gate.at[tp], local_sem.at[2]),
        pltpu.make_async_copy(up_hbm, all_up.at[tp], local_sem.at[3]),
        pltpu.make_async_copy(down_hbm, all_down.at[tp], local_sem.at[4]),
        pltpu.make_async_copy(map_hbm, pool_map, local_sem.at[5]),
        pltpu.make_async_copy(project_hbm, project, local_sem.at[6]),
    ]
    for which in (0, 5, 6, 1, 2, 3, 4):
        loads[which].start()
    docs[1 : tp_count + 1] = docs_ref[...]
    pl.semaphore_wait(barrier, experts - 1 + tp_count - 1)

    following = ((sp + 1) % experts, tp)
    prior = [
        remote(
            pool_hbm.at[tp_count - 1],
            pool_rows.at[0],
            prior_send.at[0],
            prior_recv.at[0],
            following,
        ),
        remote(
            docs_ref.at[tp_count - 1], docs.at[0], prior_send.at[1], prior_recv.at[1], following
        ),
    ]
    for copy in prior:
        copy.start()

    def region(which, block, half):
        if which == 0:
            return all_gate.at[block, pl.ds(half * depth, depth)]
        if which == 1:
            return all_up.at[block, pl.ds(half * depth, depth)]
        return all_down.at[block, :, pl.ds(half * columns, columns)]

    def own_source(which, half):
        if which == 0:
            return gate_hbm.at[pl.ds(half * depth, depth)]
        if which == 1:
            return up_hbm.at[pl.ds(half * depth, depth)]
        return down_hbm.at[:, pl.ds(half * columns, columns)]

    def own_copy(which, half, way):
        target = above if way == 0 else below
        return remote(
            own_source(which, half),
            region(which, tp, half),
            own_send.at[way, which, half],
            own_recv.at[way, which, half],
            (sp, target),
        )

    def send_own(which, half):
        for way in range(2):
            own_copy(which, half, way).start()

    def send_quarter(quarter):
        at = pl.ds(quarter * (depth // 2), depth // 2)
        for way in range(2):
            remote(
                gate_hbm.at[at],
                all_gate.at[tp, at],
                own_send.at[way, 0, 0],
                own_recv.at[way, 0, 0],
                (sp, above if way == 0 else below),
            ).start()

    def wait_own(which, half, way):
        own_copy(which, half, way).wait_recv()

    def fwd_copy(which, part, way):
        block = below if way == 0 else above
        half = 1 - way
        if which == 2:
            ref = all_down.at[block, pl.ds(half * ff_half, ff_half), pl.ds(part * columns, columns)]
        else:
            ref = region(which, block, half)
        target = above if way == 0 else below
        return remote(
            ref, ref, fwd_send.at[way, which, part], fwd_recv.at[way, which, part], (sp, target)
        )

    send_quarter(0)

    window = jnp.left_shift(jnp.int32(2), tp)
    behind = lax.broadcasted_iota(jnp.int32, (rows, rows), 0) - lax.broadcasted_iota(
        jnp.int32, (rows, rows), 1
    )
    for copy in prior:
        copy.wait_recv()
    for which in (0, 5, 6):
        loads[which].wait()

    def send_partial(owner):
        return remote(partial.at[owner], tiles.at[tp], tile_send, tile_recv, (sp, owner))

    earlier = None
    for step in (2, 1, 3, 0):
        owner = (tp + step) % tp_count
        here = jnp.broadcast_to(docs[owner + 1].astype(jnp.float32), (rows, rows))
        before = jnp.broadcast_to(docs[owner].astype(jnp.float32), (rows, rows))
        mine = here.T
        reach = jnp.where(sp * tp_count + owner > 0, window, 0)
        near = jnp.where((behind >= 0) & (behind < window) & (here == mine), 1.0, 0.0)
        far = jnp.where((behind + rows < reach) & (before == mine), 1.0, 0.0)
        counts = jnp.sum(near + far, axis=1, keepdims=True)
        current = pool_rows[owner + 1]
        running = jnp.dot(
            near.astype(jnp.bfloat16), current, preferred_element_type=jnp.float32
        ) + jnp.dot(
            far.astype(jnp.bfloat16), pool_rows[owner], preferred_element_type=jnp.float32
        )
        pooled = (running / counts - current.astype(jnp.float32)).astype(jnp.bfloat16)
        branch = (
            jnp.dot(pooled, pool_map[...], preferred_element_type=jnp.float32) * scale_ref[...]
        ).astype(jnp.bfloat16)
        block = jnp.dot(branch, project[...], preferred_element_type=jnp.float32).astype(
            jnp.bfloat16
        )
        if step:
            partial[owner] = block
        else:
            tiles[tp] = block
        if earlier is not None:
            send_partial(earlier).start()
        earlier = owner
    send_quarter(1)
    send_own(0, 1)
    send_own(1, 0)
    send_own(1, 1)

    loads[1].wait()
    summed_tiles = remote(
        tiles.at[pl.ds(0, tp_count - 1)],
        tiles.at[pl.ds(0, tp_count - 1)],
        tile_send,
        tile_recv,
        (sp, above),
    )
    summed_tiles.wait_recv()

    step_rows = 16

    @pl.loop(0, rows // step_rows)
    def _(i):
        at = pl.ds(pl.multiple_of(i * step_rows, step_rows), step_rows)
        total = tiles[0, at, :].astype(jnp.float32)
        for k in range(1, tp_count):
            total = total + tiles[k, at, :].astype(jnp.float32)
        here = (stream_v[at, :].astype(jnp.float32) + total).astype(jnp.bfloat16)
        here = here.astype(jnp.float32)
        mixed[at, :] = here
        scale = lax.rsqrt(jnp.mean(here * here, axis=1, keepdims=True) + EPS)
        normed = here * scale * gain_ref[...]
        for c in range(blocks):
            tokens[pl.ds(i * (step_rows * blocks) + c, step_rows, stride=blocks), :] = normed[
                :, c * LANES : (c + 1) * LANES
            ]

    @pl.loop(0, rows, unroll=4)
    def _(t):
        rounded[t] = tokens[pl.ds(pl.multiple_of(t * blocks, blocks), blocks), :].astype(
            jnp.bfloat16
        )

    @pl.loop(0, slots, unroll=4)
    def _(s):
        packed[s] = rounded[source_ref[s]]

    @pl.loop(1, experts)
    def _(step):
        peer = (sp + step) % experts
        remote(
            packed.at[pl.ds(peer * capacity, capacity)],
            arrived.at[pl.ds(sp * capacity, capacity)],
            row_send,
            row_recv,
            (peer, tp),
        ).start()

    @pl.loop(0, capacity)
    def _(r):
        arrived[sp * capacity + r] = packed[sp * capacity + r]

    for which in range(2):
        wait_own(which, 1, 0)
        fwd_copy(which, 0, 0).start()
        wait_own(which, 0, 1)
        fwd_copy(which, 0, 1).start()
        wait_own(which, 0, 0)
        wait_own(which, 1, 1)
    send_own(2, 0)
    send_own(2, 1)

    all_rows = remote(
        packed.at[pl.ds(0, (experts - 1) * capacity)],
        arrived.at[pl.ds(0, (experts - 1) * capacity)],
        row_send,
        row_recv,
        (sp, above),
    )
    all_rows.wait_recv()

    @pl.loop(0, slots, unroll=4)
    def _(s):
        wide[pl.ds(pl.multiple_of(s * blocks, blocks), blocks), :] = arrived[s].astype(jnp.float32)

    for c in range(blocks):
        inputs[:, c * LANES : (c + 1) * LANES] = wide[pl.ds(c, slots, stride=blocks), :].astype(
            jnp.bfloat16
        )

    loads[2].wait()
    loads[3].wait()
    loads[4].wait()

    def run_hidden(block):
        gate_pre = jnp.dot(inputs[...], all_gate[block], preferred_element_type=jnp.float32)
        up_pre = jnp.dot(inputs[...], all_up[block], preferred_element_type=jnp.float32)
        hidden[block] = (jax.nn.silu(gate_pre) * up_pre).astype(jnp.bfloat16)

    run_hidden(tp)
    run_hidden(below)
    run_hidden(above)
    for which in range(2):
        for way in range(2):
            fwd_copy(which, 0, way).wait_recv()
    run_hidden(across)

    row_step = 128
    lines = capacity * col_blocks
    for q in range(CHUNKS):
        for way in range(2):
            wait_own(2, q, way)
            fwd_copy(2, q, way).start()
        if q + 2 < CHUNKS:
            send_own(2, q + 2)
        for way in range(2):
            fwd_copy(2, q, way).wait_recv()

        @pl.loop(0, slots // row_step)
        def _(i):
            at = pl.ds(pl.multiple_of(i * row_step, row_step), row_step)
            total = jnp.zeros((row_step, columns), jnp.float32)
            for block in range(tp_count):
                piece = jnp.dot(
                    hidden[block, at, :],
                    all_down[block, :, q * columns : (q + 1) * columns],
                    preferred_element_type=jnp.float32,
                )
                total = total + piece.astype(jnp.bfloat16).astype(jnp.float32)
            for c in range(col_blocks):
                shaped[pl.ds(i * (row_step * col_blocks) + c, row_step, stride=col_blocks), :] = (
                    total[:, c * LANES : (c + 1) * LANES]
                )

        @pl.loop(0, experts)
        def _(j):
            sending[q, j] = shaped[pl.ds(pl.multiple_of(j * lines, lines), lines), :].astype(
                jnp.bfloat16
            )

        @pl.loop(1, experts)
        def _(step):
            peer = (sp + step) % experts
            remote(
                sending.at[q, peer],
                returned.at[q, sp],
                out_send.at[q],
                out_recv.at[q],
                (peer, tp),
            ).start()

        returned[q, sp] = sending[q, sp]

    def all_out(q):
        return remote(
            sending.at[q, pl.ds(0, experts - 1)],
            returned.at[q, pl.ds(0, experts - 1)],
            out_send.at[q],
            out_recv.at[q],
            (sp, above),
        )

    line = lax.broadcasted_iota(jnp.int32, (LINES, LANES), 0)
    for q in range(CHUNKS):
        all_out(q).wait_recv()
        pairs = lines // LINES

        @pl.loop(0, experts)
        def _(j):
            picked_from[pl.ds(j * pairs, pairs)] = (
                returned[q, j].astype(jnp.float32).reshape(pairs, LINES, LANES)
            )

        def picked(slot):
            tile = picked_from[slot // 2]
            return jnp.where(slot % 2 == q % 2, tile, pltpu.roll(tile, col_blocks, 0))

        @pl.loop(0, rows, unroll=4)
        def _(t):
            both = weight_ref[2 * t] * picked(slot_ref[2 * t]) + weight_ref[2 * t + 1] * picked(
                slot_ref[2 * t + 1]
            )
            at = pl.ds(pl.multiple_of(t * LINES, LINES), LINES)
            if q % 2:
                both = jnp.where(line < col_blocks, combined[at, :], both)
            combined[at, :] = both

        for c in range(col_blocks):
            at = slice(q * columns + c * LANES, q * columns + (c + 1) * LANES)
            out_ref[:, at] = (
                mixed[:, at]
                + combined[pl.ds((q % 2) * col_blocks + c, rows, stride=LINES), :]
            ).astype(jnp.bfloat16)

    for copy in prior:
        copy.wait_send()
    summed_tiles.wait_send()
    all_rows.wait_send()
    for q in range(CHUNKS):
        all_out(q).wait_send()
    for way in range(2):
        for q in range(CHUNKS):
            own_copy(2, q, way).wait_send()
            fwd_copy(2, q, way).wait_send()
        for which in range(2):
            for half in range(HALVES):
                own_copy(which, half, way).wait_send()
            fwd_copy(which, 0, way).wait_send()


def per_device(
    stream,
    pool_in,
    doc_ids,
    pool_map,
    pool_scale,
    out_weight,
    norm_gain,
    routes,
    route_weight,
    expert_gate,
    expert_up,
    expert_down,
):
    row_count = pool_in.shape[0]
    model_width = stream.shape[1]
    top_count = routes.shape[1]
    tp_count = lax.axis_size("tp")
    expert_count = lax.axis_size("sp")
    quarter = row_count // tp_count
    capacity = max(2, 3 * top_count * quarter // (2 * expert_count))
    ff_part = expert_gate.shape[2]
    own_routes = lax.dynamic_slice_in_dim(routes, lax.axis_index("tp") * quarter, quarter, 0)
    own_slots, own_sources = slot_table(own_routes, expert_count, capacity, top_count)

    slots = expert_count * capacity
    blocks = model_width // LANES
    chunk_blocks = blocks // CHUNKS
    pool_width, group_out = pool_map.shape[1:]
    bf16, f32 = jnp.bfloat16, jnp.float32
    vmem, dma = pltpu.VMEM, pltpu.SemaphoreType.DMA
    smem_spec = pl.BlockSpec(memory_space=pltpu.SMEM)
    any_spec = pl.BlockSpec(memory_space=pl.ANY)
    vmem_spec = pl.BlockSpec(memory_space=pltpu.VMEM)
    return pl.pallas_call(
        functools.partial(layer_kernel, expert_count, capacity, tp_count),
        out_shape=jax.ShapeDtypeStruct((quarter, model_width), bf16),
        in_specs=[smem_spec] * 3
        + [vmem_spec]
        + [any_spec] * 2
        + [vmem_spec]
        + [any_spec] * 2
        + [vmem_spec]
        + [any_spec] * 3,
        out_specs=vmem_spec,
        scratch_shapes=[
            vmem((tp_count + 1, quarter, pool_width), bf16),
            vmem((tp_count + 1, 1, quarter), jnp.int32),
            vmem((pool_width, group_out), bf16),
            vmem((group_out, model_width), bf16),
            vmem((tp_count, quarter, model_width), bf16),
            vmem((tp_count, quarter, model_width), bf16),
            vmem((quarter, model_width), bf16),
            vmem((quarter, model_width), f32),
            vmem((quarter * blocks, LANES), f32),
            vmem((quarter, blocks, LANES), bf16),
            vmem((slots, blocks, LANES), bf16),
            vmem((slots, blocks, LANES), bf16),
            vmem((slots * blocks, LANES), f32),
            vmem((slots, model_width), bf16),
            vmem((tp_count, model_width, ff_part), bf16),
            vmem((tp_count, model_width, ff_part), bf16),
            vmem((tp_count, ff_part, model_width), bf16),
            vmem((tp_count, slots, ff_part), bf16),
            vmem((slots * chunk_blocks, LANES), f32),
            vmem((CHUNKS, expert_count, capacity * chunk_blocks, LANES), bf16),
            vmem((CHUNKS, expert_count, capacity * chunk_blocks, LANES), bf16),
            vmem((slots * chunk_blocks // LINES, LINES, LANES), f32),
            vmem((quarter * LINES, LANES), f32),
            dma((7,)),
            dma((2,)),
            dma((2,)),
            dma,
            dma,
            dma,
            dma,
            dma((CHUNKS,)),
            dma((CHUNKS,)),
            dma((2, 3, CHUNKS)),
            dma((2, 3, CHUNKS)),
            dma((2, 3, CHUNKS)),
            dma((2, 3, CHUNKS)),
        ],
        compiler_params=pltpu.CompilerParams(
            collective_id=0, has_side_effects=True, vmem_limit_bytes=56 * 1024 * 1024
        ),
    )(
        own_sources,
        own_slots,
        route_weight.reshape(-1),
        doc_ids.reshape(tp_count, 1, quarter),
        pool_in.reshape(tp_count, quarter, pool_width),
        pool_map[0],
        pool_scale.reshape(1, -1),
        out_weight,
        stream,
        norm_gain.reshape(1, -1),
        expert_gate[0],
        expert_up[0],
        expert_down[0],
    )


def solution(mesh):
    in_specs = (
        P(("sp", "tp"), None),
        P("sp", "tp"),
        P("sp"),
        P("tp", None, None),
        P("tp"),
        P("tp", None),
        P(),
        P("sp", None),
        P(("sp", "tp"), None),
        P("sp", None, "tp"),
        P("sp", None, "tp"),
        P("sp", "tp", None),
    )
    out_specs = P(("sp", "tp"), None)
    return jax.shard_map(
        per_device, mesh=mesh, in_specs=in_specs, out_specs=out_specs, check_vma=False
    )
```

```python
import functools

import jax
import jax.numpy as jnp
from jax import lax
from jax.experimental import pallas as pl
from jax.experimental.pallas import tpu as pltpu
from jax.sharding import PartitionSpec as P

MESH = pl.DeviceIdType.MESH
EPS = 1e-06
LANES = 128
HALVES = 2
CHUNKS = 4
LINES = 8
GRID = (8, 4, 2)


def layer_kernel(
    experts,
    capacity,
    tp_count,
    grid,
    weight_ref,
    routes_ref,
    docs_ref,
    pool_hbm,
    map_hbm,
    scale_ref,
    project_hbm,
    stream_hbm,
    gain_ref,
    gate_hbm,
    up_hbm,
    down_hbm,
    out_ref,
    pool_rows,
    docs,
    pool_map,
    project,
    partial,
    relayed,
    tiles,
    stream_v,
    mixed,
    tokens,
    rounded,
    packed,
    arrived,
    wide,
    inputs,
    all_gate,
    all_up,
    all_down,
    hidden,
    shaped,
    sending,
    returned,
    picked_from,
    combined,
    table,
    table_s,
    local_sem,
    heard,
    table_sem,
    prior_send,
    prior_recv,
    relay_send,
    relay_recv,
    tile_send,
    tile_recv,
    row_send,
    row_recv,
    out_send,
    out_recv,
    own_send,
    own_recv,
    fwd_send,
    fwd_recv,
):
    sp, tp = lax.axis_index("sp"), lax.axis_index("tp")
    above, below, across = (tp + 1) % tp_count, (tp + tp_count - 1) % tp_count, (tp + 2) % tp_count
    rows, width = stream_v.shape
    blocks = width // LANES
    slots = experts * capacity
    depth = width // HALVES
    ff_part = hidden.shape[2]
    ff_half = ff_part // HALVES
    columns = width // CHUNKS
    col_blocks = columns // LANES

    def remote(src, dst, send, recv, target):
        return pltpu.make_async_remote_copy(
            src_ref=src,
            dst_ref=dst,
            send_sem=send,
            recv_sem=recv,
            device_id=target,
            device_id_type=MESH,
        )

    deep, wide_x, cores = grid
    core = sp % cores
    x_at = (sp // cores) % wide_x
    z_at = sp // (cores * wide_x)

    def plane(dz, dx, dc):
        return (
            (((z_at + dz) % deep) * wide_x + (x_at + dx) % wide_x) * cores + (core + dc) % cores,
            tp,
        )

    barrier = pltpu.get_barrier_semaphore()
    near_devices = [(sp, (tp + step) % tp_count) for step in range(1, tp_count)]
    near_devices += [plane(0, 0, 1), plane(1, 0, 0), plane(deep - 1, 0, 0)]
    near_devices += [plane(0, dx, 0) for dx in range(1, wide_x)]
    near_devices += [((sp + 1) % experts, tp), ((sp + experts - 1) % experts, tp)]
    for device in near_devices:
        pl.semaphore_signal(barrier, inc=1, device_id=device, device_id_type=MESH)

    rounds = [
        [plane(0, 0, 1)],
        [plane(1, 0, 0), plane(deep - 1, 0, 0)],
        [plane(1, 0, 0), plane(deep - 1, 0, 0)],
        [plane(2, 0, 0), plane(deep - 2, 0, 0)],
    ]

    def tell(number):
        for device in rounds[number]:
            pl.semaphore_signal(
                heard.at[number], inc=1, device_id=device, device_id_type=MESH
            )

    def hear(number):
        pl.semaphore_wait(heard.at[number], len(rounds[number]))

    loads = [
        pltpu.make_async_copy(pool_hbm, pool_rows.at[pl.ds(1, tp_count)], local_sem.at[0]),
        pltpu.make_async_copy(stream_hbm, stream_v, local_sem.at[1]),
        pltpu.make_async_copy(gate_hbm, all_gate.at[tp], local_sem.at[2]),
        pltpu.make_async_copy(up_hbm, all_up.at[tp], local_sem.at[3]),
        pltpu.make_async_copy(down_hbm, all_down.at[tp], local_sem.at[4]),
        pltpu.make_async_copy(map_hbm, pool_map, local_sem.at[5]),
        pltpu.make_async_copy(project_hbm, project, local_sem.at[6]),
    ]
    for which in (0, 5, 6, 1, 2, 3, 4):
        loads[which].start()
    docs[1 : tp_count + 1] = docs_ref[...]
    pl.semaphore_wait(barrier, len(near_devices))
    tell(0)

    following = ((sp + 1) % experts, tp)
    prior = [
        remote(
            pool_hbm.at[tp_count - 1],
            pool_rows.at[0],
            prior_send.at[0],
            prior_recv.at[0],
            following,
        ),
        remote(
            docs_ref.at[tp_count - 1], docs.at[0], prior_send.at[1], prior_recv.at[1], following
        ),
    ]
    for copy in prior:
        copy.start()

    def region(which, block, half):
        if which == 0:
            return all_gate.at[block, pl.ds(half * depth, depth)]
        if which == 1:
            return all_up.at[block, pl.ds(half * depth, depth)]
        return all_down.at[block, :, pl.ds(half * columns, columns)]

    def own_source(which, half):
        if which == 0:
            return gate_hbm.at[pl.ds(half * depth, depth)]
        if which == 1:
            return up_hbm.at[pl.ds(half * depth, depth)]
        return down_hbm.at[:, pl.ds(half * columns, columns)]

    def own_copy(which, half, way):
        target = above if way == 0 else below
        return remote(
            own_source(which, half),
            region(which, tp, half),
            own_send.at[way, which, half],
            own_recv.at[way, which, half],
            (sp, target),
        )

    def send_own(which, half):
        for way in range(2):
            own_copy(which, half, way).start()

    def send_quarter(quarter):
        at = pl.ds(quarter * (depth // 2), depth // 2)
        for way in range(2):
            remote(
                gate_hbm.at[at],
                all_gate.at[tp, at],
                own_send.at[way, 0, 0],
                own_recv.at[way, 0, 0],
                (sp, above if way == 0 else below),
            ).start()

    def wait_own(which, half, way):
        own_copy(which, half, way).wait_recv()

    def fwd_copy(which, part, way):
        block = below if way == 0 else above
        half = 1 - way
        if which == 2:
            ref = all_down.at[block, pl.ds(half * ff_half, ff_half), pl.ds(part * columns, columns)]
        else:
            ref = region(which, block, half)
        target = above if way == 0 else below
        return remote(
            ref, ref, fwd_send.at[way, which, part], fwd_recv.at[way, which, part], (sp, target)
        )

    send_quarter(0)

    def make_table():
        down_rows = lax.broadcasted_iota(jnp.int32, (rows, rows), 0)
        along = lax.broadcasted_iota(jnp.int32, (rows, rows), 1)
        at = pl.ds(pl.multiple_of(tp * rows, rows), rows)
        named = [jnp.broadcast_to(routes_ref[k : k + 1, at], (rows, rows)) for k in range(2)]
        turned = [value.T for value in named]
        found = []
        for k in range(2):
            same = jnp.where(turned[0] == named[k], 1, 0) + jnp.where(turned[1] == named[k], 1, 0)
            rank = jnp.sum(jnp.where(down_rows < along, same, 0), axis=0, keepdims=True)
            found.append(named[k][0:1, :] * capacity + rank)
            table[k : k + 1, :] = found[k]
        spread = [jnp.broadcast_to(value, (rows, rows)).T for value in found]
        for m in range(slots // LANES):
            held = (spread[0] == along + m * LANES) | (spread[1] == along + m * LANES)
            table[2 + m : 3 + m, :] = jnp.sum(
                jnp.where(held, down_rows, 0), axis=0, keepdims=True
            )
        pltpu.make_async_copy(table, table_s, table_sem).start()

    window = jnp.left_shift(jnp.int32(2), tp)
    behind = lax.broadcasted_iota(jnp.int32, (rows, rows), 0) - lax.broadcasted_iota(
        jnp.int32, (rows, rows), 1
    )
    for copy in prior:
        copy.wait_recv()
    for which in (0, 5, 6):
        loads[which].wait()

    half_rows = rows // 2

    def relay_copy(way):
        return remote(
            partial.at[across, pl.ds(way * half_rows, half_rows)],
            relayed.at[way],
            relay_send.at[way],
            relay_recv.at[way],
            (sp, above if way == 0 else below),
        )

    def tile_copy(way, half):
        owner = above if way == 0 else below
        at = pl.ds(half * half_rows, half_rows)
        return remote(
            partial.at[owner, at],
            tiles.at[way, at],
            tile_send.at[way, half],
            tile_recv.at[way, half],
            (sp, owner),
        )

    for step in (2, 1, 3, 0):
        owner = (tp + step) % tp_count
        here = jnp.broadcast_to(docs[owner + 1].astype(jnp.float32), (rows, rows))
        before = jnp.broadcast_to(docs[owner].astype(jnp.float32), (rows, rows))
        mine = here.T
        reach = jnp.where(sp * tp_count + owner > 0, window, 0)
        near = jnp.where((behind >= 0) & (behind < window) & (here == mine), 1.0, 0.0)
        far = jnp.where((behind + rows < reach) & (before == mine), 1.0, 0.0)
        counts = jnp.sum(near + far, axis=1, keepdims=True)
        current = pool_rows[owner + 1]
        running = jnp.dot(
            near.astype(jnp.bfloat16), current, preferred_element_type=jnp.float32
        ) + jnp.dot(
            far.astype(jnp.bfloat16), pool_rows[owner], preferred_element_type=jnp.float32
        )
        pooled = (running / counts - current.astype(jnp.float32)).astype(jnp.bfloat16)
        branch = (
            jnp.dot(pooled, pool_map[...], preferred_element_type=jnp.float32) * scale_ref[...]
        ).astype(jnp.bfloat16)
        block = jnp.dot(branch, project[...], preferred_element_type=jnp.float32).astype(
            jnp.bfloat16
        )
        if step:
            partial[owner] = block
        else:
            tiles[2] = block
        if step != 2:
            number = (1, 3, 0).index(step)
            hear(number)
            tell(number + 1)
        if step == 1:
            relay_copy(0).start()
            relay_copy(1).start()
        elif step == 3:
            tile_copy(0, 1).start()
        elif step == 0:
            tile_copy(1, 0).start()
    for way in range(2):
        owner = above if way == 0 else below
        at = pl.ds(way * half_rows, half_rows)
        relay_copy(way).wait_recv()
        partial[owner, at, :] = (
            partial[owner, at, :].astype(jnp.float32) + relayed[way].astype(jnp.float32)
        ).astype(jnp.bfloat16)
    make_table()
    for way in range(2):
        tile_copy(way, way).start()
    send_quarter(1)
    send_own(0, 1)
    send_own(1, 0)
    send_own(1, 1)

    loads[1].wait()
    for way in range(2):
        for half in range(2):
            tile_copy(way, half).wait_recv()

    step_rows = 16

    @pl.loop(0, rows // step_rows)
    def _(i):
        at = pl.ds(pl.multiple_of(i * step_rows, step_rows), step_rows)
        total = tiles[0, at, :].astype(jnp.float32)
        for k in range(1, 3):
            total = total + tiles[k, at, :].astype(jnp.float32)
        here = (stream_v[at, :].astype(jnp.float32) + total).astype(jnp.bfloat16)
        here = here.astype(jnp.float32)
        mixed[at, :] = here
        scale = lax.rsqrt(jnp.mean(here * here, axis=1, keepdims=True) + EPS)
        normed = here * scale * gain_ref[...]
        for c in range(blocks):
            tokens[pl.ds(i * (step_rows * blocks) + c, step_rows, stride=blocks), :] = normed[
                :, c * LANES : (c + 1) * LANES
            ]

    @pl.loop(0, rows, unroll=4)
    def _(t):
        rounded[t] = tokens[pl.ds(pl.multiple_of(t * blocks, blocks), blocks), :].astype(
            jnp.bfloat16
        )

    hear(3)
    pltpu.make_async_copy(table, table_s, table_sem).wait()

    @pl.loop(0, slots, unroll=4)
    def _(s):
        packed[s] = rounded[table_s[2 + s // LANES, s % LANES]]

    @pl.loop(1, experts)
    def _(step):
        peer = (sp + step) % experts
        remote(
            packed.at[pl.ds(peer * capacity, capacity)],
            arrived.at[pl.ds(sp * capacity, capacity)],
            row_send,
            row_recv,
            (peer, tp),
        ).start()

    @pl.loop(0, capacity)
    def _(r):
        arrived[sp * capacity + r] = packed[sp * capacity + r]

    for which in range(2):
        wait_own(which, 1, 0)
        fwd_copy(which, 0, 0).start()
        wait_own(which, 0, 1)
        fwd_copy(which, 0, 1).start()
        wait_own(which, 0, 0)
        wait_own(which, 1, 1)
    send_own(2, 0)
    send_own(2, 1)

    all_rows = remote(
        packed.at[pl.ds(0, (experts - 1) * capacity)],
        arrived.at[pl.ds(0, (experts - 1) * capacity)],
        row_send,
        row_recv,
        (sp, above),
    )
    all_rows.wait_recv()

    @pl.loop(0, slots, unroll=4)
    def _(s):
        wide[pl.ds(pl.multiple_of(s * blocks, blocks), blocks), :] = arrived[s].astype(jnp.float32)

    for c in range(blocks):
        inputs[:, c * LANES : (c + 1) * LANES] = wide[pl.ds(c, slots, stride=blocks), :].astype(
            jnp.bfloat16
        )

    loads[2].wait()
    loads[3].wait()
    loads[4].wait()

    def run_hidden(block):
        gate_pre = jnp.dot(inputs[...], all_gate[block], preferred_element_type=jnp.float32)
        up_pre = jnp.dot(inputs[...], all_up[block], preferred_element_type=jnp.float32)
        hidden[block] = (jax.nn.silu(gate_pre) * up_pre).astype(jnp.bfloat16)

    run_hidden(tp)
    run_hidden(below)
    run_hidden(above)
    for which in range(2):
        for way in range(2):
            fwd_copy(which, 0, way).wait_recv()
    run_hidden(across)

    row_step = 128
    lines = capacity * col_blocks
    for q in range(CHUNKS):
        for way in range(2):
            wait_own(2, q, way)
            fwd_copy(2, q, way).start()
        if q + 2 < CHUNKS:
            send_own(2, q + 2)
        for way in range(2):
            fwd_copy(2, q, way).wait_recv()

        @pl.loop(0, slots // row_step)
        def _(i):
            at = pl.ds(pl.multiple_of(i * row_step, row_step), row_step)
            total = jnp.zeros((row_step, columns), jnp.float32)
            for block in range(tp_count):
                piece = jnp.dot(
                    hidden[block, at, :],
                    all_down[block, :, q * columns : (q + 1) * columns],
                    preferred_element_type=jnp.float32,
                )
                total = total + piece.astype(jnp.bfloat16).astype(jnp.float32)
            for c in range(col_blocks):
                shaped[pl.ds(i * (row_step * col_blocks) + c, row_step, stride=col_blocks), :] = (
                    total[:, c * LANES : (c + 1) * LANES]
                )

        @pl.loop(0, experts)
        def _(j):
            sending[q, j] = shaped[pl.ds(pl.multiple_of(j * lines, lines), lines), :].astype(
                jnp.bfloat16
            )

        @pl.loop(1, experts)
        def _(step):
            peer = (sp + step) % experts
            remote(
                sending.at[q, peer],
                returned.at[q, sp],
                out_send.at[q],
                out_recv.at[q],
                (peer, tp),
            ).start()

        returned[q, sp] = sending[q, sp]

    def all_out(q):
        return remote(
            sending.at[q, pl.ds(0, experts - 1)],
            returned.at[q, pl.ds(0, experts - 1)],
            out_send.at[q],
            out_recv.at[q],
            (sp, above),
        )

    line = lax.broadcasted_iota(jnp.int32, (LINES, LANES), 0)
    for q in range(CHUNKS):
        all_out(q).wait_recv()
        pairs = lines // LINES

        @pl.loop(0, experts)
        def _(j):
            picked_from[pl.ds(j * pairs, pairs)] = (
                returned[q, j].astype(jnp.float32).reshape(pairs, LINES, LANES)
            )

        def picked(slot):
            tile = picked_from[slot // 2]
            return jnp.where(slot % 2 == q % 2, tile, pltpu.roll(tile, col_blocks, 0))

        @pl.loop(0, rows, unroll=4)
        def _(t):
            both = weight_ref[0, t] * picked(table_s[0, t]) + weight_ref[1, t] * picked(
                table_s[1, t]
            )
            at = pl.ds(pl.multiple_of(t * LINES, LINES), LINES)
            if q % 2:
                both = jnp.where(line < col_blocks, combined[at, :], both)
            combined[at, :] = both

        for c in range(col_blocks):
            at = slice(q * columns + c * LANES, q * columns + (c + 1) * LANES)
            out_ref[:, at] = (
                mixed[:, at]
                + combined[pl.ds((q % 2) * col_blocks + c, rows, stride=LINES), :]
            ).astype(jnp.bfloat16)

    for copy in prior:
        copy.wait_send()
    for way in range(2):
        relay_copy(way).wait_send()
        for half in range(2):
            tile_copy(way, half).wait_send()
    all_rows.wait_send()
    for q in range(CHUNKS):
        all_out(q).wait_send()
    for way in range(2):
        for q in range(CHUNKS):
            own_copy(2, q, way).wait_send()
            fwd_copy(2, q, way).wait_send()
        for which in range(2):
            for half in range(HALVES):
                own_copy(which, half, way).wait_send()
            fwd_copy(which, 0, way).wait_send()


def per_device(
    stream,
    pool_in,
    doc_ids,
    pool_map,
    pool_scale,
    out_weight,
    norm_gain,
    routes,
    route_weight,
    expert_gate,
    expert_up,
    expert_down,
):
    row_count = pool_in.shape[0]
    model_width = stream.shape[1]
    top_count = routes.shape[1]
    tp_count = lax.axis_size("tp")
    expert_count = lax.axis_size("sp")
    quarter = row_count // tp_count
    capacity = max(2, 3 * top_count * quarter // (2 * expert_count))
    ff_part = expert_gate.shape[2]
    slots = expert_count * capacity
    blocks = model_width // LANES
    chunk_blocks = blocks // CHUNKS
    pool_width, group_out = pool_map.shape[1:]
    bf16, f32 = jnp.bfloat16, jnp.float32
    vmem, dma = pltpu.VMEM, pltpu.SemaphoreType.DMA
    smem_spec = pl.BlockSpec(memory_space=pltpu.SMEM)
    any_spec = pl.BlockSpec(memory_space=pl.ANY)
    vmem_spec = pl.BlockSpec(memory_space=pltpu.VMEM)
    return pl.pallas_call(
        functools.partial(layer_kernel, expert_count, capacity, tp_count, GRID),
        out_shape=jax.ShapeDtypeStruct((quarter, model_width), bf16),
        in_specs=[smem_spec]
        + [vmem_spec] * 2
        + [any_spec] * 2
        + [vmem_spec]
        + [any_spec] * 2
        + [vmem_spec]
        + [any_spec] * 3,
        out_specs=vmem_spec,
        scratch_shapes=[
            vmem((tp_count + 1, quarter, pool_width), bf16),
            vmem((tp_count + 1, 1, quarter), jnp.int32),
            vmem((pool_width, group_out), bf16),
            vmem((group_out, model_width), bf16),
            vmem((tp_count, quarter, model_width), bf16),
            vmem((2, quarter // 2, model_width), bf16),
            vmem((3, quarter, model_width), bf16),
            vmem((quarter, model_width), bf16),
            vmem((quarter, model_width), f32),
            vmem((quarter * blocks, LANES), f32),
            vmem((quarter, blocks, LANES), bf16),
            vmem((slots, blocks, LANES), bf16),
            vmem((slots, blocks, LANES), bf16),
            vmem((slots * blocks, LANES), f32),
            vmem((slots, model_width), bf16),
            vmem((tp_count, model_width, ff_part), bf16),
            vmem((tp_count, model_width, ff_part), bf16),
            vmem((tp_count, ff_part, model_width), bf16),
            vmem((tp_count, slots, ff_part), bf16),
            vmem((slots * chunk_blocks, LANES), f32),
            vmem((CHUNKS, expert_count, capacity * chunk_blocks, LANES), bf16),
            vmem((CHUNKS, expert_count, capacity * chunk_blocks, LANES), bf16),
            vmem((slots * chunk_blocks // LINES, LINES, LANES), f32),
            vmem((quarter * LINES, LANES), f32),
            vmem((8, LANES), jnp.int32),
            pltpu.SMEM((8, LANES), jnp.int32),
            dma((7,)),
            pltpu.SemaphoreType.REGULAR((4,)),
            dma,
            dma((2,)),
            dma((2,)),
            dma((2,)),
            dma((2,)),
            dma((2, 2)),
            dma((2, 2)),
            dma,
            dma,
            dma((CHUNKS,)),
            dma((CHUNKS,)),
            dma((2, 3, CHUNKS)),
            dma((2, 3, CHUNKS)),
            dma((2, 3, CHUNKS)),
            dma((2, 3, CHUNKS)),
        ],
        compiler_params=pltpu.CompilerParams(
            collective_id=0, has_side_effects=True, vmem_limit_bytes=56 * 1024 * 1024
        ),
    )(
        route_weight.T,
        routes.T,
        doc_ids.reshape(tp_count, 1, quarter),
        pool_in.reshape(tp_count, quarter, pool_width),
        pool_map[0],
        pool_scale.reshape(1, -1),
        out_weight,
        stream,
        norm_gain.reshape(1, -1),
        expert_gate[0],
        expert_up[0],
        expert_down[0],
    )


def solution(mesh):
    in_specs = (
        P(("sp", "tp"), None),
        P("sp", "tp"),
        P("sp"),
        P("tp", None, None),
        P("tp"),
        P("tp", None),
        P(),
        P("sp", None),
        P(("sp", "tp"), None),
        P("sp", None, "tp"),
        P("sp", None, "tp"),
        P("sp", "tp", None),
    )
    out_specs = P(("sp", "tp"), None)
    return jax.shard_map(
        per_device, mesh=mesh, in_specs=in_specs, out_specs=out_specs, check_vma=False
    )
```

```python
import functools

import jax
import jax.numpy as jnp
from jax import lax
from jax.experimental import pallas as pl
from jax.experimental.pallas import tpu as pltpu
from jax.sharding import PartitionSpec as P

MESH = pl.DeviceIdType.MESH
EPS = 1e-06
LANES = 128
HALVES = 2
CHUNKS = 4
LINES = 8
GRID = (8, 4, 2)


def layer_kernel(
    experts,
    capacity,
    tp_count,
    grid,
    weight_ref,
    routes_ref,
    docs_ref,
    pool_hbm,
    map_hbm,
    scale_ref,
    project_hbm,
    stream_hbm,
    gain_ref,
    gate_hbm,
    up_hbm,
    down_hbm,
    out_ref,
    pool_rows,
    docs,
    pool_map,
    project,
    partial,
    relayed,
    tiles,
    stream_v,
    mixed,
    tokens,
    rounded,
    packed,
    arrived,
    wide,
    inputs,
    all_gate,
    all_up,
    all_down,
    hidden,
    shaped,
    sending,
    returned,
    picked_from,
    combined,
    table,
    table_s,
    local_sem,
    heard,
    table_sem,
    prior_send,
    prior_recv,
    relay_send,
    relay_recv,
    tile_send,
    tile_recv,
    row_send,
    row_recv,
    out_send,
    out_recv,
    own_send,
    own_recv,
    fwd_send,
    fwd_recv,
):
    sp, tp = lax.axis_index("sp"), lax.axis_index("tp")
    above, below, across = (tp + 1) % tp_count, (tp + tp_count - 1) % tp_count, (tp + 2) % tp_count
    rows, width = stream_v.shape
    blocks = width // LANES
    slots = experts * capacity
    depth = width // HALVES
    ff_part = hidden.shape[2]
    ff_half = ff_part // HALVES
    columns = width // CHUNKS
    col_blocks = columns // LANES

    def remote(src, dst, send, recv, target):
        return pltpu.make_async_remote_copy(
            src_ref=src,
            dst_ref=dst,
            send_sem=send,
            recv_sem=recv,
            device_id=target,
            device_id_type=MESH,
        )

    deep, wide_x, cores = grid
    core = sp % cores
    x_at = (sp // cores) % wide_x
    z_at = sp // (cores * wide_x)

    def plane(dz, dx, dc):
        return (
            (((z_at + dz) % deep) * wide_x + (x_at + dx) % wide_x) * cores + (core + dc) % cores,
            tp,
        )

    barrier = pltpu.get_barrier_semaphore()
    near_devices = [(sp, (tp + step) % tp_count) for step in range(1, tp_count)]
    near_devices += [plane(0, 0, 1), plane(1, 0, 0), plane(deep - 1, 0, 0)]
    near_devices += [plane(0, dx, 0) for dx in range(1, wide_x)]
    near_devices += [((sp + 1) % experts, tp), ((sp + experts - 1) % experts, tp)]
    for device in near_devices:
        pl.semaphore_signal(barrier, inc=1, device_id=device, device_id_type=MESH)

    rounds = [
        [plane(0, 0, 1)],
        [plane(1, 0, 0), plane(deep - 1, 0, 0)],
        [plane(1, 0, 0), plane(deep - 1, 0, 0)],
        [plane(2, 0, 0), plane(deep - 2, 0, 0)],
    ]

    def tell(number):
        for device in rounds[number]:
            pl.semaphore_signal(
                heard.at[number], inc=1, device_id=device, device_id_type=MESH
            )

    def hear(number):
        pl.semaphore_wait(heard.at[number], len(rounds[number]))

    loads = [
        pltpu.make_async_copy(pool_hbm, pool_rows.at[pl.ds(1, tp_count)], local_sem.at[0]),
        pltpu.make_async_copy(stream_hbm, stream_v, local_sem.at[1]),
        pltpu.make_async_copy(gate_hbm, all_gate.at[tp], local_sem.at[2]),
        pltpu.make_async_copy(up_hbm, all_up.at[tp], local_sem.at[3]),
        pltpu.make_async_copy(down_hbm, all_down.at[tp], local_sem.at[4]),
        pltpu.make_async_copy(map_hbm, pool_map, local_sem.at[5]),
        pltpu.make_async_copy(project_hbm, project, local_sem.at[6]),
    ]
    for which in (0, 5, 6, 1, 2, 3, 4):
        loads[which].start()
    docs[1 : tp_count + 1] = docs_ref[...]
    pl.semaphore_wait(barrier, len(near_devices))
    tell(0)

    following = ((sp + 1) % experts, tp)
    prior = [
        remote(
            pool_hbm.at[tp_count - 1],
            pool_rows.at[0],
            prior_send.at[0],
            prior_recv.at[0],
            following,
        ),
        remote(
            docs_ref.at[tp_count - 1], docs.at[0], prior_send.at[1], prior_recv.at[1], following
        ),
    ]
    for copy in prior:
        copy.start()

    def region(which, block, half):
        if which == 0:
            return all_gate.at[block, pl.ds(half * depth, depth)]
        if which == 1:
            return all_up.at[block, pl.ds(half * depth, depth)]
        return all_down.at[block, :, pl.ds(half * columns, columns)]

    def own_source(which, half):
        if which == 0:
            return gate_hbm.at[pl.ds(half * depth, depth)]
        if which == 1:
            return up_hbm.at[pl.ds(half * depth, depth)]
        return down_hbm.at[:, pl.ds(half * columns, columns)]

    def own_copy(which, half, way):
        target = above if way == 0 else below
        return remote(
            own_source(which, half),
            region(which, tp, half),
            own_send.at[way, which, half],
            own_recv.at[way, which, half],
            (sp, target),
        )

    def send_own(which, half):
        for way in range(2):
            own_copy(which, half, way).start()

    def send_quarter(quarter):
        at = pl.ds(quarter * (depth // 2), depth // 2)
        for way in range(2):
            remote(
                gate_hbm.at[at],
                all_gate.at[tp, at],
                own_send.at[way, 0, 0],
                own_recv.at[way, 0, 0],
                (sp, above if way == 0 else below),
            ).start()

    def wait_own(which, half, way):
        own_copy(which, half, way).wait_recv()

    def fwd_copy(which, part, way):
        block = below if way == 0 else above
        half = 1 - way
        if which == 2:
            ref = all_down.at[block, pl.ds(half * ff_half, ff_half), pl.ds(part * columns, columns)]
        else:
            ref = region(which, block, half)
        target = above if way == 0 else below
        return remote(
            ref, ref, fwd_send.at[way, which, part], fwd_recv.at[way, which, part], (sp, target)
        )

    send_quarter(0)

    def make_table():
        down_rows = lax.broadcasted_iota(jnp.int32, (rows, rows), 0)
        along = lax.broadcasted_iota(jnp.int32, (rows, rows), 1)
        at = pl.ds(pl.multiple_of(tp * rows, rows), rows)
        named = [jnp.broadcast_to(routes_ref[k : k + 1, at], (rows, rows)) for k in range(2)]
        turned = [value.T for value in named]
        found = []
        for k in range(2):
            same = jnp.where(turned[0] == named[k], 1, 0) + jnp.where(turned[1] == named[k], 1, 0)
            rank = jnp.sum(jnp.where(down_rows < along, same, 0), axis=0, keepdims=True)
            found.append(named[k][0:1, :] * capacity + rank)
            table[k : k + 1, :] = found[k]
        spread = [jnp.broadcast_to(value, (rows, rows)).T for value in found]
        for m in range(slots // LANES):
            held = (spread[0] == along + m * LANES) | (spread[1] == along + m * LANES)
            table[2 + m : 3 + m, :] = jnp.sum(
                jnp.where(held, down_rows, 0), axis=0, keepdims=True
            )
        pltpu.make_async_copy(table, table_s, table_sem).start()

    window = jnp.left_shift(jnp.int32(2), tp)
    behind = lax.broadcasted_iota(jnp.int32, (rows, rows), 0) - lax.broadcasted_iota(
        jnp.int32, (rows, rows), 1
    )
    for copy in prior:
        copy.wait_recv()
    for which in (0, 5, 6):
        loads[which].wait()

    half_rows = rows // 2

    def relay_copy(way):
        return remote(
            partial.at[across, pl.ds(way * half_rows, half_rows)],
            relayed.at[way],
            relay_send.at[way],
            relay_recv.at[way],
            (sp, above if way == 0 else below),
        )

    def tile_copy(way, half):
        owner = above if way == 0 else below
        at = pl.ds(half * half_rows, half_rows)
        return remote(
            partial.at[owner, at],
            tiles.at[way, at],
            tile_send.at[way, half],
            tile_recv.at[way, half],
            (sp, owner),
        )

    for step in (2, 1, 3, 0):
        owner = (tp + step) % tp_count
        here = jnp.broadcast_to(docs[owner + 1].astype(jnp.float32), (rows, rows))
        before = jnp.broadcast_to(docs[owner].astype(jnp.float32), (rows, rows))
        mine = here.T
        reach = jnp.where(sp * tp_count + owner > 0, window, 0)
        near = jnp.where((behind >= 0) & (behind < window) & (here == mine), 1.0, 0.0)
        far = jnp.where((behind + rows < reach) & (before == mine), 1.0, 0.0)
        counts = jnp.sum(near + far, axis=1, keepdims=True)
        current = pool_rows[owner + 1]
        running = jnp.dot(
            near.astype(jnp.bfloat16), current, preferred_element_type=jnp.float32
        ) + jnp.dot(
            far.astype(jnp.bfloat16), pool_rows[owner], preferred_element_type=jnp.float32
        )
        pooled = (running / counts - current.astype(jnp.float32)).astype(jnp.bfloat16)
        branch = (
            jnp.dot(pooled, pool_map[...], preferred_element_type=jnp.float32) * scale_ref[...]
        ).astype(jnp.bfloat16)
        block = jnp.dot(branch, project[...], preferred_element_type=jnp.float32).astype(
            jnp.bfloat16
        )
        if step:
            partial[owner] = block
        else:
            tiles[2] = block
        if step != 2:
            number = (1, 3, 0).index(step)
            hear(number)
            tell(number + 1)
        if step == 1:
            relay_copy(0).start()
            relay_copy(1).start()
        elif step == 3:
            tile_copy(0, 1).start()
        elif step == 0:
            tile_copy(1, 0).start()
    for way in range(2):
        owner = above if way == 0 else below
        at = pl.ds(way * half_rows, half_rows)
        relay_copy(way).wait_recv()
        partial[owner, at, :] = (
            partial[owner, at, :].astype(jnp.float32) + relayed[way].astype(jnp.float32)
        ).astype(jnp.bfloat16)
    make_table()
    for way in range(2):
        tile_copy(way, way).start()
    send_quarter(1)
    send_own(0, 1)
    send_own(1, 0)
    send_own(1, 1)

    loads[1].wait()
    for way in range(2):
        for half in range(2):
            tile_copy(way, half).wait_recv()

    step_rows = 16

    @pl.loop(0, rows // step_rows)
    def _(i):
        at = pl.ds(pl.multiple_of(i * step_rows, step_rows), step_rows)
        total = tiles[0, at, :].astype(jnp.float32)
        for k in range(1, 3):
            total = total + tiles[k, at, :].astype(jnp.float32)
        here = (stream_v[at, :].astype(jnp.float32) + total).astype(jnp.bfloat16)
        here = here.astype(jnp.float32)
        mixed[at, :] = here
        scale = lax.rsqrt(jnp.mean(here * here, axis=1, keepdims=True) + EPS)
        normed = here * scale * gain_ref[...]
        for c in range(blocks):
            tokens[pl.ds(i * (step_rows * blocks) + c, step_rows, stride=blocks), :] = normed[
                :, c * LANES : (c + 1) * LANES
            ]

    @pl.loop(0, rows, unroll=4)
    def _(t):
        rounded[t] = tokens[pl.ds(pl.multiple_of(t * blocks, blocks), blocks), :].astype(
            jnp.bfloat16
        )

    hear(3)
    pltpu.make_async_copy(table, table_s, table_sem).wait()

    @pl.loop(0, slots, unroll=4)
    def _(s):
        packed[s] = rounded[table_s[2 + s // LANES, s % LANES]]

    @pl.loop(1, experts, unroll=7)
    def _(step):
        peer = (sp + step) % experts
        remote(
            packed.at[pl.ds(peer * capacity, capacity)],
            arrived.at[pl.ds(sp * capacity, capacity)],
            row_send,
            row_recv,
            (peer, tp),
        ).start()

    @pl.loop(0, capacity)
    def _(r):
        arrived[sp * capacity + r] = packed[sp * capacity + r]

    for which in range(2):
        wait_own(which, 1, 0)
        fwd_copy(which, 0, 0).start()
        wait_own(which, 0, 1)
        fwd_copy(which, 0, 1).start()
        wait_own(which, 0, 0)
        wait_own(which, 1, 1)
    send_own(2, 0)
    send_own(2, 1)

    all_rows = remote(
        packed.at[pl.ds(0, (experts - 1) * capacity)],
        arrived.at[pl.ds(0, (experts - 1) * capacity)],
        row_send,
        row_recv,
        (sp, above),
    )
    all_rows.wait_recv()

    @pl.loop(0, slots, unroll=4)
    def _(s):
        wide[pl.ds(pl.multiple_of(s * blocks, blocks), blocks), :] = arrived[s].astype(jnp.float32)

    for c in range(blocks):
        inputs[:, c * LANES : (c + 1) * LANES] = wide[pl.ds(c, slots, stride=blocks), :].astype(
            jnp.bfloat16
        )

    loads[2].wait()
    loads[3].wait()
    loads[4].wait()

    def run_hidden(block):
        gate_pre = jnp.dot(inputs[...], all_gate[block], preferred_element_type=jnp.float32)
        up_pre = jnp.dot(inputs[...], all_up[block], preferred_element_type=jnp.float32)
        hidden[block] = (jax.nn.silu(gate_pre) * up_pre).astype(jnp.bfloat16)

    run_hidden(tp)
    run_hidden(below)
    run_hidden(above)
    for which in range(2):
        for way in range(2):
            fwd_copy(which, 0, way).wait_recv()
    run_hidden(across)

    row_step = 128
    lines = capacity * col_blocks

    def pass_down(q):
        for way in range(2):
            wait_own(2, q, way)
            fwd_copy(2, q, way).start()
        if q + 2 < CHUNKS:
            send_own(2, q + 2)

    pass_down(0)
    for q in range(CHUNKS):
        if q + 1 < CHUNKS:
            pass_down(q + 1)
        for way in range(2):
            fwd_copy(2, q, way).wait_recv()

        @pl.loop(0, slots // row_step)
        def _(i):
            at = pl.ds(pl.multiple_of(i * row_step, row_step), row_step)
            total = jnp.zeros((row_step, columns), jnp.float32)
            for block in range(tp_count):
                piece = jnp.dot(
                    hidden[block, at, :],
                    all_down[block, :, q * columns : (q + 1) * columns],
                    preferred_element_type=jnp.float32,
                )
                total = total + piece.astype(jnp.bfloat16).astype(jnp.float32)
            for c in range(col_blocks):
                shaped[pl.ds(i * (row_step * col_blocks) + c, row_step, stride=col_blocks), :] = (
                    total[:, c * LANES : (c + 1) * LANES]
                )

        @pl.loop(0, experts, unroll=8)
        def _(j):
            sending[q, j] = shaped[pl.ds(pl.multiple_of(j * lines, lines), lines), :].astype(
                jnp.bfloat16
            )

        @pl.loop(1, experts, unroll=7)
        def _(step):
            peer = (sp + step) % experts
            remote(
                sending.at[q, peer],
                returned.at[q, sp],
                out_send.at[q],
                out_recv.at[q],
                (peer, tp),
            ).start()

        returned[q, sp] = sending[q, sp]

    def all_out(q):
        return remote(
            sending.at[q, pl.ds(0, experts - 1)],
            returned.at[q, pl.ds(0, experts - 1)],
            out_send.at[q],
            out_recv.at[q],
            (sp, above),
        )

    line = lax.broadcasted_iota(jnp.int32, (LINES, LANES), 0)
    for q in range(CHUNKS):
        all_out(q).wait_recv()
        pairs = lines // LINES

        @pl.loop(0, experts, unroll=8)
        def _(j):
            picked_from[pl.ds(j * pairs, pairs)] = (
                returned[q, j].astype(jnp.float32).reshape(pairs, LINES, LANES)
            )

        def picked(slot):
            tile = picked_from[slot // 2]
            return jnp.where(slot % 2 == q % 2, tile, pltpu.roll(tile, col_blocks, 0))

        @pl.loop(0, rows, unroll=16)
        def _(t):
            both = weight_ref[0, t] * picked(table_s[0, t]) + weight_ref[1, t] * picked(
                table_s[1, t]
            )
            at = pl.ds(pl.multiple_of(t * LINES, LINES), LINES)
            if q % 2:
                both = jnp.where(line < col_blocks, combined[at, :], both)
            combined[at, :] = both

        for c in range(col_blocks):
            at = slice(q * columns + c * LANES, q * columns + (c + 1) * LANES)
            out_ref[:, at] = (
                mixed[:, at]
                + combined[pl.ds((q % 2) * col_blocks + c, rows, stride=LINES), :]
            ).astype(jnp.bfloat16)

    for copy in prior:
        copy.wait_send()
    for way in range(2):
        relay_copy(way).wait_send()
        for half in range(2):
            tile_copy(way, half).wait_send()
    all_rows.wait_send()
    for q in range(CHUNKS):
        all_out(q).wait_send()
    for way in range(2):
        for q in range(CHUNKS):
            own_copy(2, q, way).wait_send()
            fwd_copy(2, q, way).wait_send()
        for which in range(2):
            for half in range(HALVES):
                own_copy(which, half, way).wait_send()
            fwd_copy(which, 0, way).wait_send()


def per_device(
    stream,
    pool_in,
    doc_ids,
    pool_map,
    pool_scale,
    out_weight,
    norm_gain,
    routes,
    route_weight,
    expert_gate,
    expert_up,
    expert_down,
):
    row_count = pool_in.shape[0]
    model_width = stream.shape[1]
    top_count = routes.shape[1]
    tp_count = lax.axis_size("tp")
    expert_count = lax.axis_size("sp")
    quarter = row_count // tp_count
    capacity = max(2, 3 * top_count * quarter // (2 * expert_count))
    ff_part = expert_gate.shape[2]
    slots = expert_count * capacity
    blocks = model_width // LANES
    chunk_blocks = blocks // CHUNKS
    pool_width, group_out = pool_map.shape[1:]
    bf16, f32 = jnp.bfloat16, jnp.float32
    vmem, dma = pltpu.VMEM, pltpu.SemaphoreType.DMA
    smem_spec = pl.BlockSpec(memory_space=pltpu.SMEM)
    any_spec = pl.BlockSpec(memory_space=pl.ANY)
    vmem_spec = pl.BlockSpec(memory_space=pltpu.VMEM)
    return pl.pallas_call(
        functools.partial(layer_kernel, expert_count, capacity, tp_count, GRID),
        out_shape=pltpu.VMEM((quarter, model_width), bf16),
        in_specs=[smem_spec]
        + [vmem_spec] * 2
        + [any_spec] * 2
        + [vmem_spec]
        + [any_spec] * 2
        + [vmem_spec]
        + [any_spec] * 3,
        out_specs=vmem_spec,
        scratch_shapes=[
            vmem((tp_count + 1, quarter, pool_width), bf16),
            vmem((tp_count + 1, 1, quarter), jnp.int32),
            vmem((pool_width, group_out), bf16),
            vmem((group_out, model_width), bf16),
            vmem((tp_count, quarter, model_width), bf16),
            vmem((2, quarter // 2, model_width), bf16),
            vmem((3, quarter, model_width), bf16),
            vmem((quarter, model_width), bf16),
            vmem((quarter, model_width), f32),
            vmem((quarter * blocks, LANES), f32),
            vmem((quarter, blocks, LANES), bf16),
            vmem((slots, blocks, LANES), bf16),
            vmem((slots, blocks, LANES), bf16),
            vmem((slots * blocks, LANES), f32),
            vmem((slots, model_width), bf16),
            vmem((tp_count, model_width, ff_part), bf16),
            vmem((tp_count, model_width, ff_part), bf16),
            vmem((tp_count, ff_part, model_width), bf16),
            vmem((tp_count, slots, ff_part), bf16),
            vmem((slots * chunk_blocks, LANES), f32),
            vmem((CHUNKS, expert_count, capacity * chunk_blocks, LANES), bf16),
            vmem((CHUNKS, expert_count, capacity * chunk_blocks, LANES), bf16),
            vmem((slots * chunk_blocks // LINES, LINES, LANES), f32),
            vmem((quarter * LINES, LANES), f32),
            vmem((8, LANES), jnp.int32),
            pltpu.SMEM((8, LANES), jnp.int32),
            dma((7,)),
            pltpu.SemaphoreType.REGULAR((4,)),
            dma,
            dma((2,)),
            dma((2,)),
            dma((2,)),
            dma((2,)),
            dma((2, 2)),
            dma((2, 2)),
            dma,
            dma,
            dma((CHUNKS,)),
            dma((CHUNKS,)),
            dma((2, 3, CHUNKS)),
            dma((2, 3, CHUNKS)),
            dma((2, 3, CHUNKS)),
            dma((2, 3, CHUNKS)),
        ],
        compiler_params=pltpu.CompilerParams(
            collective_id=0, has_side_effects=True, vmem_limit_bytes=56 * 1024 * 1024
        ),
    )(
        route_weight.T,
        routes.T,
        doc_ids.reshape(tp_count, 1, quarter),
        pool_in.reshape(tp_count, quarter, pool_width),
        pool_map[0],
        pool_scale.reshape(1, -1),
        out_weight,
        stream,
        norm_gain.reshape(1, -1),
        expert_gate[0],
        expert_up[0],
        expert_down[0],
    )


def solution(mesh):
    in_specs = (
        P(("sp", "tp"), None),
        P("sp", "tp"),
        P("sp"),
        P("tp", None, None),
        P("tp"),
        P("tp", None),
        P(),
        P("sp", None),
        P(("sp", "tp"), None),
        P("sp", None, "tp"),
        P("sp", None, "tp"),
        P("sp", "tp", None),
    )
    out_specs = P(("sp", "tp"), None)
    return jax.shard_map(
        per_device, mesh=mesh, in_specs=in_specs, out_specs=out_specs, check_vma=False
    )
```

```python
import functools

import jax
import jax.numpy as jnp
from jax import lax
from jax.experimental import pallas as pl
from jax.experimental.pallas import tpu as pltpu
from jax.sharding import PartitionSpec as P

MESH = pl.DeviceIdType.MESH
EPS = 1e-06
LANES = 128
HALVES = 2
CHUNKS = 4
LINES = 8
GRID = (8, 4, 2)


def layer_kernel(
    experts,
    capacity,
    tp_count,
    grid,
    weight_ref,
    routes_ref,
    docs_ref,
    pool_hbm,
    map_hbm,
    scale_ref,
    project_hbm,
    stream_hbm,
    gain_ref,
    gate_hbm,
    up_hbm,
    down_hbm,
    out_ref,
    pool_rows,
    docs,
    pool_map,
    project,
    partial,
    relayed,
    tiles,
    stream_v,
    mixed,
    tokens,
    rounded,
    packed,
    arrived,
    wide,
    inputs,
    all_gate,
    all_up,
    all_down,
    hidden,
    shaped,
    sending,
    returned,
    picked_from,
    combined,
    early,
    table,
    table_s,
    local_sem,
    heard,
    table_sem,
    prior_send,
    prior_recv,
    relay_send,
    relay_recv,
    tile_send,
    tile_recv,
    row_send,
    row_recv,
    out_send,
    out_recv,
    own_send,
    own_recv,
    fwd_send,
    fwd_recv,
):
    sp, tp = lax.axis_index("sp"), lax.axis_index("tp")
    above, below, across = (tp + 1) % tp_count, (tp + tp_count - 1) % tp_count, (tp + 2) % tp_count
    rows, width = stream_v.shape
    blocks = width // LANES
    slots = experts * capacity
    depth = width // HALVES
    ff_part = hidden.shape[2]
    ff_half = ff_part // HALVES
    columns = width // CHUNKS
    col_blocks = columns // LANES

    def remote(src, dst, send, recv, target):
        return pltpu.make_async_remote_copy(
            src_ref=src,
            dst_ref=dst,
            send_sem=send,
            recv_sem=recv,
            device_id=target,
            device_id_type=MESH,
        )

    deep, wide_x, cores = grid
    core = sp % cores
    x_at = (sp // cores) % wide_x
    z_at = sp // (cores * wide_x)

    def plane(dz, dx, dc):
        return (
            (((z_at + dz) % deep) * wide_x + (x_at + dx) % wide_x) * cores + (core + dc) % cores,
            tp,
        )

    barrier = pltpu.get_barrier_semaphore()
    near_devices = [(sp, (tp + step) % tp_count) for step in range(1, tp_count)]
    near_devices += [plane(0, 0, 1), plane(1, 0, 0), plane(deep - 1, 0, 0)]
    near_devices += [plane(0, dx, 0) for dx in range(1, wide_x)]
    near_devices += [((sp + 1) % experts, tp), ((sp + experts - 1) % experts, tp)]
    for device in near_devices:
        pl.semaphore_signal(barrier, inc=1, device_id=device, device_id_type=MESH)

    rounds = [
        [plane(0, 0, 1)],
        [plane(1, 0, 0), plane(deep - 1, 0, 0)],
        [plane(1, 0, 0), plane(deep - 1, 0, 0)],
        [plane(2, 0, 0), plane(deep - 2, 0, 0)],
    ]

    def tell(number):
        for device in rounds[number]:
            pl.semaphore_signal(
                heard.at[number], inc=1, device_id=device, device_id_type=MESH
            )

    def hear(number):
        pl.semaphore_wait(heard.at[number], len(rounds[number]))

    loads = [
        pltpu.make_async_copy(pool_hbm, pool_rows.at[pl.ds(1, tp_count)], local_sem.at[0]),
        pltpu.make_async_copy(stream_hbm, stream_v, local_sem.at[1]),
        pltpu.make_async_copy(gate_hbm, all_gate.at[tp], local_sem.at[2]),
        pltpu.make_async_copy(up_hbm, all_up.at[tp], local_sem.at[3]),
        pltpu.make_async_copy(down_hbm, all_down.at[tp], local_sem.at[4]),
        pltpu.make_async_copy(map_hbm, pool_map, local_sem.at[5]),
        pltpu.make_async_copy(project_hbm, project, local_sem.at[6]),
    ]
    for which in (0, 5, 6, 1, 2, 3, 4):
        loads[which].start()
    docs[1 : tp_count + 1] = docs_ref[...]
    pl.semaphore_wait(barrier, len(near_devices))
    tell(0)

    following = ((sp + 1) % experts, tp)
    prior = [
        remote(
            pool_hbm.at[tp_count - 1],
            pool_rows.at[0],
            prior_send.at[0],
            prior_recv.at[0],
            following,
        ),
        remote(
            docs_ref.at[tp_count - 1], docs.at[0], prior_send.at[1], prior_recv.at[1], following
        ),
    ]
    for copy in prior:
        copy.start()

    def region(which, block, half):
        if which == 0:
            return all_gate.at[block, pl.ds(half * depth, depth)]
        if which == 1:
            return all_up.at[block, pl.ds(half * depth, depth)]
        return all_down.at[block, :, pl.ds(half * columns, columns)]

    def own_source(which, half):
        if which == 0:
            return gate_hbm.at[pl.ds(half * depth, depth)]
        if which == 1:
            return up_hbm.at[pl.ds(half * depth, depth)]
        return down_hbm.at[:, pl.ds(half * columns, columns)]

    def own_copy(which, half, way):
        target = above if way == 0 else below
        return remote(
            own_source(which, half),
            region(which, tp, half),
            own_send.at[way, which, half],
            own_recv.at[way, which, half],
            (sp, target),
        )

    def send_own(which, half):
        for way in range(2):
            own_copy(which, half, way).start()

    def send_quarter(quarter):
        at = pl.ds(quarter * (depth // 2), depth // 2)
        for way in range(2):
            remote(
                gate_hbm.at[at],
                all_gate.at[tp, at],
                own_send.at[way, 0, 0],
                own_recv.at[way, 0, 0],
                (sp, above if way == 0 else below),
            ).start()

    def wait_own(which, half, way):
        own_copy(which, half, way).wait_recv()

    def fwd_copy(which, part, way):
        block = below if way == 0 else above
        half = 1 - way
        if which == 2:
            ref = all_down.at[block, pl.ds(half * ff_half, ff_half), pl.ds(part * columns, columns)]
        else:
            ref = region(which, block, half)
        target = above if way == 0 else below
        return remote(
            ref, ref, fwd_send.at[way, which, part], fwd_recv.at[way, which, part], (sp, target)
        )

    send_quarter(0)

    def make_table():
        down_rows = lax.broadcasted_iota(jnp.int32, (rows, rows), 0)
        along = lax.broadcasted_iota(jnp.int32, (rows, rows), 1)
        at = pl.ds(pl.multiple_of(tp * rows, rows), rows)
        named = [jnp.broadcast_to(routes_ref[k : k + 1, at], (rows, rows)) for k in range(2)]
        turned = [value.T for value in named]
        found = []
        for k in range(2):
            same = jnp.where(turned[0] == named[k], 1, 0) + jnp.where(turned[1] == named[k], 1, 0)
            rank = jnp.sum(jnp.where(down_rows < along, same, 0), axis=0, keepdims=True)
            found.append(named[k][0:1, :] * capacity + rank)
            table[k : k + 1, :] = found[k]
        spread = [jnp.broadcast_to(value, (rows, rows)).T for value in found]
        for m in range(slots // LANES):
            held = (spread[0] == along + m * LANES) | (spread[1] == along + m * LANES)
            table[2 + m : 3 + m, :] = jnp.sum(
                jnp.where(held, down_rows, 0), axis=0, keepdims=True
            )
        pltpu.make_async_copy(table, table_s, table_sem).start()

    window = jnp.left_shift(jnp.int32(2), tp)
    behind = lax.broadcasted_iota(jnp.int32, (rows, rows), 0) - lax.broadcasted_iota(
        jnp.int32, (rows, rows), 1
    )
    for copy in prior:
        copy.wait_recv()
    for which in (0, 5, 6):
        loads[which].wait()

    half_rows = rows // 2

    def relay_copy(way):
        return remote(
            partial.at[across, pl.ds(way * half_rows, half_rows)],
            relayed.at[way],
            relay_send.at[way],
            relay_recv.at[way],
            (sp, above if way == 0 else below),
        )

    def tile_copy(way, half):
        owner = above if way == 0 else below
        at = pl.ds(half * half_rows, half_rows)
        return remote(
            partial.at[owner, at],
            tiles.at[way, at],
            tile_send.at[way, half],
            tile_recv.at[way, half],
            (sp, owner),
        )

    for step in (2, 1, 3, 0):
        owner = (tp + step) % tp_count
        here = jnp.broadcast_to(docs[owner + 1].astype(jnp.float32), (rows, rows))
        before = jnp.broadcast_to(docs[owner].astype(jnp.float32), (rows, rows))
        mine = here.T
        reach = jnp.where(sp * tp_count + owner > 0, window, 0)
        near = jnp.where((behind >= 0) & (behind < window) & (here == mine), 1.0, 0.0)
        far = jnp.where((behind + rows < reach) & (before == mine), 1.0, 0.0)
        counts = jnp.sum(near + far, axis=1, keepdims=True)
        current = pool_rows[owner + 1]
        running = jnp.dot(
            near.astype(jnp.bfloat16), current, preferred_element_type=jnp.float32
        ) + jnp.dot(
            far.astype(jnp.bfloat16), pool_rows[owner], preferred_element_type=jnp.float32
        )
        pooled = (running / counts - current.astype(jnp.float32)).astype(jnp.bfloat16)
        branch = (
            jnp.dot(pooled, pool_map[...], preferred_element_type=jnp.float32) * scale_ref[...]
        ).astype(jnp.bfloat16)
        block = jnp.dot(branch, project[...], preferred_element_type=jnp.float32).astype(
            jnp.bfloat16
        )
        if step:
            partial[owner] = block
        else:
            tiles[2] = block
        if step != 2:
            number = (1, 3, 0).index(step)
            hear(number)
            tell(number + 1)
        if step == 1:
            relay_copy(0).start()
            relay_copy(1).start()
        elif step == 3:
            tile_copy(0, 1).start()
        elif step == 0:
            tile_copy(1, 0).start()
    for way in range(2):
        owner = above if way == 0 else below
        at = pl.ds(way * half_rows, half_rows)
        relay_copy(way).wait_recv()
        partial[owner, at, :] = (
            partial[owner, at, :].astype(jnp.float32) + relayed[way].astype(jnp.float32)
        ).astype(jnp.bfloat16)
    for way in range(2):
        tile_copy(way, way).start()
    send_quarter(1)
    send_own(0, 1)
    send_own(1, 0)
    send_own(1, 1)
    make_table()

    loads[1].wait()
    for way in range(2):
        for half in range(2):
            tile_copy(way, half).wait_recv()

    step_rows = 16

    @pl.loop(0, rows // step_rows)
    def _(i):
        at = pl.ds(pl.multiple_of(i * step_rows, step_rows), step_rows)
        total = tiles[0, at, :].astype(jnp.float32)
        for k in range(1, 3):
            total = total + tiles[k, at, :].astype(jnp.float32)
        here = (stream_v[at, :].astype(jnp.float32) + total).astype(jnp.bfloat16)
        here = here.astype(jnp.float32)
        mixed[at, :] = here
        scale = lax.rsqrt(jnp.mean(here * here, axis=1, keepdims=True) + EPS)
        normed = here * scale * gain_ref[...]
        for c in range(blocks):
            tokens[pl.ds(i * (step_rows * blocks) + c, step_rows, stride=blocks), :] = normed[
                :, c * LANES : (c + 1) * LANES
            ]

    @pl.loop(0, rows, unroll=4)
    def _(t):
        rounded[t] = tokens[pl.ds(pl.multiple_of(t * blocks, blocks), blocks), :].astype(
            jnp.bfloat16
        )

    hear(3)
    pltpu.make_async_copy(table, table_s, table_sem).wait()

    @pl.loop(0, slots, unroll=4)
    def _(s):
        packed[s] = rounded[table_s[2 + s // LANES, s % LANES]]

    @pl.loop(1, experts, unroll=7)
    def _(step):
        peer = (sp + step) % experts
        remote(
            packed.at[pl.ds(peer * capacity, capacity)],
            arrived.at[pl.ds(sp * capacity, capacity)],
            row_send,
            row_recv,
            (peer, tp),
        ).start()

    @pl.loop(0, capacity)
    def _(r):
        arrived[sp * capacity + r] = packed[sp * capacity + r]

    for which in range(2):
        wait_own(which, 1, 0)
        fwd_copy(which, 0, 0).start()
        wait_own(which, 0, 1)
        fwd_copy(which, 0, 1).start()
        wait_own(which, 0, 0)
        wait_own(which, 1, 1)
    send_own(2, 0)
    send_own(2, 1)

    all_rows = remote(
        packed.at[pl.ds(0, (experts - 1) * capacity)],
        arrived.at[pl.ds(0, (experts - 1) * capacity)],
        row_send,
        row_recv,
        (sp, above),
    )
    all_rows.wait_recv()

    @pl.loop(0, slots, unroll=4)
    def _(s):
        wide[pl.ds(pl.multiple_of(s * blocks, blocks), blocks), :] = arrived[s].astype(jnp.float32)

    for c in range(blocks):
        inputs[:, c * LANES : (c + 1) * LANES] = wide[pl.ds(c, slots, stride=blocks), :].astype(
            jnp.bfloat16
        )

    loads[2].wait()
    loads[3].wait()
    loads[4].wait()

    def run_hidden(block):
        gate_pre = jnp.dot(inputs[...], all_gate[block], preferred_element_type=jnp.float32)
        up_pre = jnp.dot(inputs[...], all_up[block], preferred_element_type=jnp.float32)
        hidden[block] = (jax.nn.silu(gate_pre) * up_pre).astype(jnp.bfloat16)

    run_hidden(tp)
    run_hidden(below)
    run_hidden(above)
    for which in range(2):
        for way in range(2):
            fwd_copy(which, 0, way).wait_recv()
    run_hidden(across)

    row_step = 128
    lines = capacity * col_blocks

    def pass_down(q):
        for way in range(2):
            wait_own(2, q, way)
            fwd_copy(2, q, way).start()
        if q + 2 < CHUNKS:
            send_own(2, q + 2)

    pass_down(0)
    for q in range(CHUNKS):
        if q + 1 < CHUNKS:
            pass_down(q + 1)
        def down_part(block, at):
            return (
                jnp.dot(
                    hidden[block, at, :],
                    all_down[block, :, q * columns : (q + 1) * columns],
                    preferred_element_type=jnp.float32,
                )
                .astype(jnp.bfloat16)
                .astype(jnp.float32)
            )

        @pl.loop(0, slots // row_step)
        def _(i):
            at = pl.ds(pl.multiple_of(i * row_step, row_step), row_step)
            early[at, :] = down_part(tp, at) + down_part(below, at) + down_part(above, at)

        for way in range(2):
            fwd_copy(2, q, way).wait_recv()

        @pl.loop(0, slots // row_step)
        def _(i):
            at = pl.ds(pl.multiple_of(i * row_step, row_step), row_step)
            total = early[at, :] + down_part(across, at)
            for c in range(col_blocks):
                shaped[pl.ds(i * (row_step * col_blocks) + c, row_step, stride=col_blocks), :] = (
                    total[:, c * LANES : (c + 1) * LANES]
                )

        @pl.loop(0, experts, unroll=8)
        def _(j):
            sending[q, j] = shaped[pl.ds(pl.multiple_of(j * lines, lines), lines), :].astype(
                jnp.bfloat16
            )

        @pl.loop(1, experts, unroll=7)
        def _(step):
            peer = (sp + step) % experts
            remote(
                sending.at[q, peer],
                returned.at[q, sp],
                out_send.at[q],
                out_recv.at[q],
                (peer, tp),
            ).start()

        returned[q, sp] = sending[q, sp]

    def all_out(q):
        return remote(
            sending.at[q, pl.ds(0, experts - 1)],
            returned.at[q, pl.ds(0, experts - 1)],
            out_send.at[q],
            out_recv.at[q],
            (sp, above),
        )

    line = lax.broadcasted_iota(jnp.int32, (LINES, LANES), 0)
    for q in range(CHUNKS):
        all_out(q).wait_recv()
        pairs = lines // LINES

        @pl.loop(0, experts, unroll=8)
        def _(j):
            picked_from[pl.ds(j * pairs, pairs)] = (
                returned[q, j].astype(jnp.float32).reshape(pairs, LINES, LANES)
            )

        def picked(slot):
            tile = picked_from[slot // 2]
            return jnp.where(slot % 2 == q % 2, tile, pltpu.roll(tile, col_blocks, 0))

        @pl.loop(0, rows, unroll=16)
        def _(t):
            both = weight_ref[0, t] * picked(table_s[0, t]) + weight_ref[1, t] * picked(
                table_s[1, t]
            )
            at = pl.ds(pl.multiple_of(t * LINES, LINES), LINES)
            if q % 2:
                both = jnp.where(line < col_blocks, combined[at, :], both)
            combined[at, :] = both

        for c in range(col_blocks):
            at = slice(q * columns + c * LANES, q * columns + (c + 1) * LANES)
            out_ref[:, at] = (
                mixed[:, at]
                + combined[pl.ds((q % 2) * col_blocks + c, rows, stride=LINES), :]
            ).astype(jnp.bfloat16)

    for copy in prior:
        copy.wait_send()
    for way in range(2):
        relay_copy(way).wait_send()
        for half in range(2):
            tile_copy(way, half).wait_send()
    all_rows.wait_send()
    for q in range(CHUNKS):
        all_out(q).wait_send()
    for way in range(2):
        for q in range(CHUNKS):
            own_copy(2, q, way).wait_send()
            fwd_copy(2, q, way).wait_send()
        for which in range(2):
            for half in range(HALVES):
                own_copy(which, half, way).wait_send()
            fwd_copy(which, 0, way).wait_send()


def per_device(
    stream,
    pool_in,
    doc_ids,
    pool_map,
    pool_scale,
    out_weight,
    norm_gain,
    routes,
    route_weight,
    expert_gate,
    expert_up,
    expert_down,
):
    row_count = pool_in.shape[0]
    model_width = stream.shape[1]
    top_count = routes.shape[1]
    tp_count = lax.axis_size("tp")
    expert_count = lax.axis_size("sp")
    quarter = row_count // tp_count
    capacity = max(2, 3 * top_count * quarter // (2 * expert_count))
    ff_part = expert_gate.shape[2]
    slots = expert_count * capacity
    blocks = model_width // LANES
    chunk_blocks = blocks // CHUNKS
    pool_width, group_out = pool_map.shape[1:]
    bf16, f32 = jnp.bfloat16, jnp.float32
    vmem, dma = pltpu.VMEM, pltpu.SemaphoreType.DMA
    smem_spec = pl.BlockSpec(memory_space=pltpu.SMEM)
    any_spec = pl.BlockSpec(memory_space=pl.ANY)
    vmem_spec = pl.BlockSpec(memory_space=pltpu.VMEM)
    return pl.pallas_call(
        functools.partial(layer_kernel, expert_count, capacity, tp_count, GRID),
        out_shape=pltpu.VMEM((quarter, model_width), bf16),
        in_specs=[smem_spec]
        + [vmem_spec] * 2
        + [any_spec] * 2
        + [vmem_spec]
        + [any_spec] * 2
        + [vmem_spec]
        + [any_spec] * 3,
        out_specs=vmem_spec,
        scratch_shapes=[
            vmem((tp_count + 1, quarter, pool_width), bf16),
            vmem((tp_count + 1, 1, quarter), jnp.int32),
            vmem((pool_width, group_out), bf16),
            vmem((group_out, model_width), bf16),
            vmem((tp_count, quarter, model_width), bf16),
            vmem((2, quarter // 2, model_width), bf16),
            vmem((3, quarter, model_width), bf16),
            vmem((quarter, model_width), bf16),
            vmem((quarter, model_width), f32),
            vmem((quarter * blocks, LANES), f32),
            vmem((quarter, blocks, LANES), bf16),
            vmem((slots, blocks, LANES), bf16),
            vmem((slots, blocks, LANES), bf16),
            vmem((slots * blocks, LANES), f32),
            vmem((slots, model_width), bf16),
            vmem((tp_count, model_width, ff_part), bf16),
            vmem((tp_count, model_width, ff_part), bf16),
            vmem((tp_count, ff_part, model_width), bf16),
            vmem((tp_count, slots, ff_part), bf16),
            vmem((slots * chunk_blocks, LANES), f32),
            vmem((CHUNKS, expert_count, capacity * chunk_blocks, LANES), bf16),
            vmem((CHUNKS, expert_count, capacity * chunk_blocks, LANES), bf16),
            vmem((slots * chunk_blocks // LINES, LINES, LANES), f32),
            vmem((quarter * LINES, LANES), f32),
            vmem((slots, model_width // CHUNKS), f32),
            vmem((8, LANES), jnp.int32),
            pltpu.SMEM((8, LANES), jnp.int32),
            dma((7,)),
            pltpu.SemaphoreType.REGULAR((4,)),
            dma,
            dma((2,)),
            dma((2,)),
            dma((2,)),
            dma((2,)),
            dma((2, 2)),
            dma((2, 2)),
            dma,
            dma,
            dma((CHUNKS,)),
            dma((CHUNKS,)),
            dma((2, 3, CHUNKS)),
            dma((2, 3, CHUNKS)),
            dma((2, 3, CHUNKS)),
            dma((2, 3, CHUNKS)),
        ],
        compiler_params=pltpu.CompilerParams(
            collective_id=0, has_side_effects=True, vmem_limit_bytes=56 * 1024 * 1024
        ),
    )(
        route_weight.T,
        routes.T,
        doc_ids.reshape(tp_count, 1, quarter),
        pool_in.reshape(tp_count, quarter, pool_width),
        pool_map[0],
        pool_scale.reshape(1, -1),
        out_weight,
        stream,
        norm_gain.reshape(1, -1),
        expert_gate[0],
        expert_up[0],
        expert_down[0],
    )


def solution(mesh):
    in_specs = (
        P(("sp", "tp"), None),
        P("sp", "tp"),
        P("sp"),
        P("tp", None, None),
        P("tp"),
        P("tp", None),
        P(),
        P("sp", None),
        P(("sp", "tp"), None),
        P("sp", None, "tp"),
        P("sp", None, "tp"),
        P("sp", "tp", None),
    )
    out_specs = P(("sp", "tp"), None)
    return jax.shard_map(
        per_device, mesh=mesh, in_specs=in_specs, out_specs=out_specs, check_vma=False
    )
```
